32 devices in a mesh: sp: 16 (over z, y, x), tp: 2 (over core).
Axes of the slice: x: 2, y: 2, z: 4, core: 2. Of those that a mesh axis runs over, the one named last changes fastest.
Arguments:
- residual: bfloat16 [3072, 2048], P(('sp', 'tp')), may hold values from -6 to 6
- queries: bfloat16 [3072, 1024], P('sp', 'tp'), may hold values from -6 to 6
- key_pairs: bfloat16 [3072, 1024], P('sp', 'tp'), may hold values from -6 to 6
- values: bfloat16 [3072, 1024], P('sp', 'tp'), may hold values from -6 to 6
- second_weight: float32 [8], P('tp'), may hold values from 0.3 to 0.8
- head_gain: float32 [1024], P('tp'), may hold values from 0.1 to 1.9
- out_weight: bfloat16 [1024, 2048], P('tp'), may hold values from -0.1875 to 0.1875
- norm_gain: float32 [2048], replicated, may hold values from 0.1 to 1.9
- up_weight: bfloat16 [2048, 5632], P('sp', 'tp'), may hold values from -0.125 to 0.125
- gate_weight: bfloat16 [2048, 5632], P('sp', 'tp'), may hold values from -0.125 to 0.125
- conv_weight: float32 [3, 5632], P(None, 'tp'), may hold values from -3.5 to 3.5
- conv_bias: float32 [5632], P('tp'), may hold values from -3 to 3
- down_weight: bfloat16 [5632, 2048], P('tp', 'sp'), may hold values from -0.078125 to 0.078125
Outputs:
- layer_out: bfloat16 [3072, 2048], P(('sp', 'tp'))
The draws below stay inside these ranges and needn't reach their ends.
All inputs are finite; a program needn't handle non-finite values.
Results may differ from the reference program's by a relative error of at most 0.017.
Values may be sent and summed in bfloat16 or wider, within the bound.
A program may use at most 128 MiB of HBM per device.

```python
import math
import jax
import jax.numpy as jnp
from jax import lax

D = 2048
HEADS = 8
HD = 64
VD = 128
FF = 5632
KW = 3
TOKENS = 3072
N_TP = 2


def plant_pairs(key):
    base_key = jax.random.fold_in(key, 101)
    key_q, key_k = jax.random.split(base_key, 2)
    width_all = HEADS * 2 * HD
    query_draw = jax.random.normal(key_q, (TOKENS, width_all), jnp.float32) * 1.3
    key_draw = jax.random.normal(key_k, (TOKENS, width_all), jnp.float32) * 1.3
    return (jnp.clip(query_draw, -6.0, 6.0), jnp.clip(key_draw, -6.0, 6.0))


def draw_queries(key, part):
    return plant_pairs(key)[0].astype(jnp.bfloat16)


def draw_key_pairs(key, part):
    return plant_pairs(key)[1].astype(jnp.bfloat16)


def steps_of(stream_key, extent, cuts, least, high):
    loudness = 1.0
    for position, blocks in cuts:
        draws = jax.random.uniform(jax.random.fold_in(jax.random.fold_in(stream_key, 6), position), (blocks,), jnp.float32, least / len(cuts), high / len(cuts))
        loudness = loudness * jnp.repeat(jnp.exp(draws), extent[position] // blocks).reshape((-1,) + (1,) * (len(extent) - 1 - position))
    return loudness


def normal_values(key, extent, spread, bound, cuts=(), held_as=jnp.bfloat16):
    entries = jax.random.normal(key, extent, jnp.float32) * spread
    if len(cuts) > 0:
        entries = steps_of(key, extent, cuts, -0.22, 0.18) * entries
    return jnp.clip(entries, min=-bound, max=bound).astype(held_as)


def setup_inputs(seed: int = 0) -> dict:
    key_list = jax.random.split(jax.random.key(seed), 14)
    return {
        "residual": normal_values(key_list[0], (TOKENS, D), 1.0, 6.0, ((0, 32),)),
        "queries": draw_queries(jax.random.fold_in(key_list[13], 71), 0),
        "key_pairs": draw_key_pairs(jax.random.fold_in(key_list[13], 71), 0),
        "values": normal_values(key_list[3], (TOKENS, HEADS * VD), 1.0, 6.0, ((0, 16), (1, 2))),
        "second_weight": jnp.clip(0.3 + 0.5 * jax.random.uniform(key_list[4], (HEADS,), jnp.float32) ** steps_of(key_list[4], (HEADS,), ((0, 2),), -0.2, 0.2), 0.3, 0.8),
        "head_gain": jnp.clip(1.0 + 0.18 * jax.random.normal(key_list[5], (HEADS * VD,), jnp.float32), 0.1, 1.9),
        "out_weight": normal_values(key_list[6], (HEADS * VD, D), (HEADS * VD) ** -0.5, 0.1875, ((0, 2),)),
        "norm_gain": jnp.clip(1.0 + 0.18 * jax.random.normal(key_list[7], (D,), jnp.float32), 0.1, 1.9),
        "up_weight": normal_values(key_list[8], (D, FF), D ** -0.5, 0.125, ((0, 16), (1, 2))),
        "gate_weight": normal_values(key_list[9], (D, FF), D ** -0.5, 0.125, ((0, 16), (1, 2))),
        "conv_weight": normal_values(key_list[10], (KW, FF), KW ** -0.5, 3.5, ((1, 2),), jnp.float32),
        "conv_bias": normal_values(key_list[11], (FF,), 0.5, 3.0, ((0, 2),), jnp.float32),
        "down_weight": normal_values(key_list[12], (FF, D), FF ** -0.5, 0.078125, ((0, 2), (1, 16))),
    }


eps = 1e-05
neg_fill = -1e+30

def normalize(rows_in, gain):
    values_f = rows_in.astype(jnp.float32)
    scale_inv = lax.rsqrt(lax.optimization_barrier(jnp.mean(values_f * values_f, axis=-1, keepdims=True)) + eps)
    return (values_f * scale_inv * gain).astype(jnp.bfloat16)

def reference(residual, queries, key_pairs, values, second_weight, head_gain, out_weight, norm_gain, up_weight, gate_weight, conv_weight, conv_bias, down_weight):
    block_size = math.gcd(TOKENS, 512)
    block_count = TOKENS // block_size
    query_all = queries.astype(jnp.float32).reshape(TOKENS, HEADS, 2, HD)
    key_all = key_pairs.astype(jnp.float32).reshape(TOKENS, HEADS, 2, HD)
    value_all = values.astype(jnp.float32).reshape(TOKENS, HEADS, VD)
    key_pos = jnp.arange(TOKENS).astype(jnp.int32)
    gain_heads = head_gain.reshape(HEADS, VD)

    def attend_block(index_block):
        first = (index_block * block_size).astype(jnp.int32)
        query_block = lax.dynamic_slice_in_dim(query_all, first, block_size, 0)
        positions = first + jnp.arange(block_size).astype(jnp.int32)
        scores = jnp.einsum('qhmd,khmd->hmqk', query_block, key_all) * HD ** (-0.5)
        visible = key_pos[None, :] <= positions[:, None]
        scores = jnp.where(visible, scores, neg_fill)
        maxima = lax.optimization_barrier(jnp.max(scores, axis=-1, keepdims=True))
        exp_scores = jnp.where(visible, jnp.exp(scores - maxima), jnp.float32(0.0))
        totals = lax.optimization_barrier(jnp.sum(exp_scores, axis=-1))
        rounded = exp_scores.astype(jnp.bfloat16).astype(jnp.float32)
        weighted = jnp.einsum('hmqk,khe->hmqe', rounded, value_all)
        diff = weighted[:, 0] / totals[:, 0, :, None] - second_weight[:, None, None] * weighted[:, 1] / totals[:, 1, :, None]
        diff = jnp.transpose(diff, (1, 0, 2))
        scale_inv = lax.rsqrt(lax.optimization_barrier(jnp.mean(diff * diff, axis=-1, keepdims=True)) + eps)
        normed_heads = diff * scale_inv * gain_heads * 0.8
        return normed_heads.reshape(block_size, HEADS * VD).astype(jnp.bfloat16)
    attended = lax.map(attend_block, jnp.arange(block_count).astype(jnp.int32)).reshape(TOKENS, HEADS * VD)
    group_rows = HEADS * VD // N_TP
    proj_sum = jnp.zeros((TOKENS, D), jnp.float32)
    for group in range(N_TP):
        part_prod = jnp.dot(attended[:, group * group_rows:(group + 1) * group_rows], out_weight[group * group_rows:(group + 1) * group_rows], preferred_element_type=jnp.float32)
        proj_sum = proj_sum + part_prod.astype(jnp.bfloat16).astype(jnp.float32)
    proj = proj_sum.astype(jnp.bfloat16)
    mid = (residual.astype(jnp.float32) + proj.astype(jnp.float32)).astype(jnp.bfloat16)
    normed = normalize(mid, norm_gain)
    up_proj = jnp.dot(normed, up_weight, preferred_element_type=jnp.float32).astype(jnp.bfloat16)
    gate_proj = jnp.dot(normed, gate_weight, preferred_element_type=jnp.float32).astype(jnp.bfloat16)
    padded = jnp.pad(up_proj.astype(jnp.float32), ((KW - 1, 0), (0, 0)))
    conv_out = jnp.zeros((TOKENS, FF), jnp.float32) + conv_bias
    for tap in range(KW):
        conv_out = conv_out + conv_weight[tap] * padded[tap:tap + TOKENS]
    hidden = (jax.nn.silu(conv_out) * gate_proj.astype(jnp.float32)).astype(jnp.bfloat16)
    group_units = FF // N_TP
    ffn_sum = jnp.zeros((TOKENS, D), jnp.float32)
    for group in range(N_TP):
        part_prod = jnp.dot(hidden[:, group * group_units:(group + 1) * group_units], down_weight[group * group_units:(group + 1) * group_units], preferred_element_type=jnp.float32)
        ffn_sum = ffn_sum + part_prod.astype(jnp.bfloat16).astype(jnp.float32)
    ffn_out = ffn_sum.astype(jnp.bfloat16)
    return (mid.astype(jnp.float32) + ffn_out.astype(jnp.float32)).astype(jnp.bfloat16)
```

```python
import functools

import jax
import jax.numpy as jnp
from jax import lax
from jax.experimental import pallas as pl
from jax.experimental.pallas import tpu as pltpu
from jax.sharding import PartitionSpec as P

MESH = pl.DeviceIdType.MESH
VMEM_LIMIT = 60 * 1024 * 1024

HD = 64
VD = 128


eps = 1e-05
neg_fill = -1e30


def from_behind(value, axis, steps):
    count = lax.axis_size(axis)
    leading, last = (max(0, -steps), min(count, count - steps))
    return lax.ppermute(value, axis, [(source, source + steps) for source in range(leading, last)])


def normalize(rows_in, gain):
    values_f = rows_in.astype(jnp.float32)
    scale_inv = lax.rsqrt(jnp.mean(values_f * values_f, axis=-1, keepdims=True) + eps)
    return (values_f * scale_inv * gain).astype(jnp.bfloat16)


def attend(queries, key_pairs, values, second_weight, head_gain):
    tok_rows = queries.shape[0]
    head_count = second_weight.shape[0]
    sp_index = lax.axis_index("sp")
    query = queries.reshape(tok_rows, head_count, 2, HD)
    query_pos = sp_index * tok_rows + jnp.arange(tok_rows)
    last_query = (sp_index + 1) * tok_rows
    initial = (
        jnp.full((head_count, 2, tok_rows), neg_fill, jnp.float32),
        jnp.zeros((head_count, 2, tok_rows), jnp.float32),
        jnp.zeros((head_count, 2, tok_rows, VD), jnp.float32),
    )
    key_piece = lax.all_gather(key_pairs, "sp", axis=0, tiled=True)
    value_piece = lax.all_gather(values, "sp", axis=0, tiled=True)
    piece_len = key_piece.shape[0]

    def compute(state_in):
        maxima, totals, weighted = state_in
        key_rows = key_piece.reshape(piece_len, head_count, 2, HD)
        value_rows = value_piece.reshape(piece_len, head_count, VD)
        scores = jnp.einsum(
            "qhmd,khmd->hmqk", query, key_rows, preferred_element_type=jnp.float32
        ) * HD ** (-0.5)
        visible = jnp.arange(piece_len)[None, :] <= query_pos[:, None]
        scores = jnp.where(visible, scores, neg_fill)
        new_max = jnp.maximum(maxima, jnp.max(scores, axis=-1))
        exp_scores = jnp.where(visible, jnp.exp(scores - new_max[..., None]), jnp.float32(0.0))
        totals = jnp.sum(exp_scores, axis=-1)
        weighted = jnp.einsum(
            "hmqk,khe->hmqe",
            exp_scores.astype(jnp.bfloat16),
            value_rows,
            preferred_element_type=jnp.float32,
        )
        return (new_max, totals, weighted)

    def keep_state(state_in):
        return state_in

    maxima, totals, weighted = lax.cond(jnp.int32(0) < last_query, compute, keep_state, initial)
    diff = (
        weighted[:, 0] / totals[:, 0, :, None]
        - second_weight[:, None, None] * weighted[:, 1] / totals[:, 1, :, None]
    )
    diff = jnp.transpose(diff, (1, 0, 2))
    scale_inv = lax.rsqrt(jnp.mean(diff * diff, axis=-1, keepdims=True) + eps)
    attended = (
        (diff * scale_inv * head_gain.reshape(head_count, VD) * 0.8)
        .reshape(tok_rows, head_count * VD)
        .astype(jnp.bfloat16)
    )
    return attended


def local(
    residual,
    queries,
    key_pairs,
    values,
    second_weight,
    head_gain,
    out_weight,
    norm_gain,
    up_weight,
    gate_weight,
    conv_weight,
    conv_bias,
    down_weight,
):
    tok_rows = queries.shape[0]
    ff_local = up_weight.shape[1]
    attended = attend(queries, key_pairs, values, second_weight, head_gain)
    proj = lax.psum_scatter(
        jnp.dot(attended, out_weight, preferred_element_type=jnp.float32).astype(jnp.bfloat16),
        "tp",
        scatter_dimension=0,
        tiled=True,
    )
    mid = (residual.astype(jnp.float32) + proj.astype(jnp.float32)).astype(jnp.bfloat16)
    normed_all = lax.all_gather(normalize(mid, norm_gain), "tp", axis=0, tiled=True)
    up_sum = jnp.dot(
        normed_all,
        lax.all_gather(up_weight, "sp", axis=0, tiled=True),
        preferred_element_type=jnp.float32,
    )
    gate_sum = jnp.dot(
        normed_all,
        lax.all_gather(gate_weight, "sp", axis=0, tiled=True),
        preferred_element_type=jnp.float32,
    )
    up_proj = up_sum.astype(jnp.bfloat16)
    gate_proj = gate_sum.astype(jnp.bfloat16)
    taps = conv_weight.shape[0]
    rim_rows = from_behind(up_proj[tok_rows - (taps - 1) :], "sp", 1)
    extended = jnp.concatenate((rim_rows, up_proj), axis=0)
    conv_out = jnp.zeros((tok_rows, ff_local), jnp.float32) + conv_bias[None, :]
    for tap in range(taps):
        conv_out = conv_out + conv_weight[tap][None, :] * extended[tap : tap + tok_rows].astype(
            jnp.float32
        )
    hidden = (jax.nn.silu(conv_out) * gate_proj.astype(jnp.float32)).astype(jnp.bfloat16)
    down_all = lax.all_gather(down_weight, "sp", axis=1, tiled=True)
    ffn_out = lax.psum_scatter(
        jnp.dot(hidden, down_all, preferred_element_type=jnp.float32).astype(jnp.bfloat16),
        "tp",
        scatter_dimension=0,
        tiled=True,
    )
    return (mid.astype(jnp.float32) + ffn_out.astype(jnp.float32)).astype(jnp.bfloat16)


def greet(n, me, t):
    barrier = pltpu.get_barrier_semaphore()

    def signal(k, carry):
        pl.semaphore_signal(
            barrier, inc=1, device_id={"sp": lax.rem(me + k, n)}, device_id_type=MESH
        )
        return carry

    lax.fori_loop(1, n, signal, 0)
    pl.semaphore_signal(barrier, inc=1, device_id={"tp": 1 - t}, device_id_type=MESH)
    pl.semaphore_wait(barrier, n)


def to_sp(src, dst, send, recv, dest):
    return pltpu.make_async_remote_copy(
        src_ref=src, dst_ref=dst, send_sem=send, recv_sem=recv,
        device_id={"sp": dest}, device_id_type=MESH,
    )


def to_tp(src, dst, send, recv, dest):
    return pltpu.make_async_remote_copy(
        src_ref=src, dst_ref=dst, send_sem=send, recv_sem=recv,
        device_id={"tp": dest}, device_id_type=MESH,
    )


def span(index, size):
    return pl.ds(pl.multiple_of(index * size, size), size)


def first_tile(group, tiles, groups):
    return group * tiles // groups


def tile_count(tiles, groups):
    return -(-tiles // groups)


class Place:
    def __init__(self, n):
        self.n = n
        self.layers = n // 4
        self.me = lax.axis_index("sp")
        self.t = lax.axis_index("tp")
        self.z = self.me // 4
        self.w = lax.rem(self.me, 4)
        self.y = self.w // 2
        self.x = lax.rem(self.w, 2)
        self.xn = self.z * 4 + self.y * 2 + (1 - self.x)
        self.yn = self.z * 4 + (1 - self.y) * 2 + self.x

    def ahead(self, a):
        return lax.rem(self.z + a, self.layers)

    def behind(self, a):
        return lax.rem(self.z - a + self.layers, self.layers)

    def chip(self, z, y, x):
        return z * 4 + y * 2 + x


def attention_kernel(
    n, q, k, v, sw, gain, ow, res, ngain, uw, gw, dw,
    mid, normed, wu, wg, wd,
    qb, kb, vb, ob, sb, att, pbuf, prbuf,
    zsend, zrecv, psend, precv, osend, orecv, tsem, wsend, wrecv, fsend, frecv,
):
    here = Place(n)
    me, t, z, w, y, x = here.me, here.t, here.z, here.w, here.y, here.x
    layers = here.layers
    rows = q.shape[0]
    half = rows // 2
    depth = uw.shape[0]
    groups = n // 2
    tiles = uw.shape[1] // VD
    wide = wu.shape[1]
    chunk = 4 * rows
    greet(n, me, t)

    def cols(h):
        return span(h, VD)

    def along_z(a):
        zz = here.ahead(a)
        dest = here.chip(zz, y, x)
        return (
            to_sp(k.at[:, cols(zz)], kb.at[span(me, rows)], zsend.at[0, a], zrecv.at[0, a], dest),
            to_sp(v.at[:, cols(zz)], vb.at[span(me, rows)], zsend.at[1, a], zrecv.at[1, a], dest),
            to_sp(q.at[:, cols(zz)], qb.at[z], zsend.at[2, a], zrecv.at[2, a], dest),
        )

    def in_plane(a):
        own = span(here.behind(a) * 4 + w, rows)
        return (
            to_sp(kb.at[own], kb.at[own], psend.at[0, a], precv.at[0, a], here.xn),
            to_sp(vb.at[own], vb.at[own], psend.at[1, a], precv.at[1, a], here.yn),
            to_sp(vb.at[own], vb.at[own], psend.at[2, a], precv.at[2, a], here.xn),
            to_sp(kb.at[own], kb.at[own], psend.at[3, a], precv.at[3, a], here.yn),
        )

    def corner(a):
        from_x = span(here.chip(here.behind(a), y, 1 - x), rows)
        from_y = span(here.chip(here.behind(a), 1 - y, x), rows)
        return (
            to_sp(kb.at[from_x], kb.at[from_x], psend.at[4, a], precv.at[4, a], here.yn),
            to_sp(vb.at[from_y], vb.at[from_y], psend.at[5, a], precv.at[5, a], here.xn),
        )

    def weights(a, b):
        slot = a * 2 + b
        zz = here.ahead(a)
        yy = lax.rem(y + b, 2)
        dest = here.chip(zz, yy, x)
        first = pl.multiple_of(first_tile(zz * 2 + yy, tiles, groups) * VD, VD)
        part = pl.ds(first, wide)
        mine = span(me, depth)
        return (
            to_sp(uw.at[:, part], wu.at[mine], wsend.at[0, slot], wrecv.at[0, slot], dest),
            to_sp(gw.at[:, part], wg.at[mine], wsend.at[1, slot], wrecv.at[1, slot], dest),
            to_sp(dw.at[part], wd.at[:, mine], wsend.at[2, slot], wrecv.at[2, slot], dest),
        )

    def across_x(a, b):
        slot = a * 2 + b
        got = span(here.chip(here.behind(a), lax.rem(y + b, 2), x), depth)
        return (
            to_sp(wu.at[got], wu.at[got], fsend.at[0, slot], frecv.at[0, slot], here.xn),
            to_sp(wg.at[got], wg.at[got], fsend.at[1, slot], frecv.at[1, slot], here.xn),
            to_sp(
                wd.at[:, got], wd.at[:, got], fsend.at[2, slot], frecv.at[2, slot], here.xn
            ),
        )

    def pass_on(a, b):
        for copy in weights(a, b):
            copy.wait_recv()
        for copy in across_x(a, b):
            copy.start()

    for a in range(1, layers):
        for copy in along_z(a):
            copy.start()
    kb[span(me, rows), :] = k[:, cols(z)]
    vb[span(me, rows), :] = v[:, cols(z)]
    qb[z] = q[:, cols(z)]
    for copy in in_plane(0):
        copy.start()
    for a in range(1, layers):
        for copy in weights(a, 0):
            copy.start()
    for copy in weights(0, 1):
        copy.start()
    own_first = pl.multiple_of(first_tile(z * 2 + y, tiles, groups) * VD, VD)
    own_part = pl.ds(own_first, wide)
    wu[span(me, depth), :] = uw[:, own_part]
    wg[span(me, depth), :] = gw[:, own_part]
    wd[:, span(me, depth)] = dw[own_part, :]

    def corner_stage(a):
        in_plane(a)[0].wait_recv()
        corner(a)[0].start()
        in_plane(a)[1].wait_recv()
        corner(a)[1].start()

    def stage(a, carry):
        copies = along_z(a)
        copies[0].wait_recv()
        copies[1].wait_recv()
        for copy in in_plane(a):
            copy.start()
        corner_stage(a - 1)
        return carry

    lax.fori_loop(1, layers, stage, 0)
    corner_stage(layers - 1)
    for copy in across_x(0, 0):
        copy.start()

    def settle(a, carry):
        in_plane(a)[2].wait_recv()
        in_plane(a)[3].wait_recv()
        corner(a)[0].wait_recv()
        corner(a)[1].wait_recv()
        return carry

    lax.fori_loop(0, layers, settle, 0)
    for a in range(1, layers):
        along_z(a)[2].wait_recv()

    weight = sw[z]
    gain_row = gain[pl.ds(z, 1), :]
    lane = lax.broadcasted_iota(jnp.int32, (rows, VD), 1)

    def answer(i):
        return to_sp(
            ob.at[i], att.at[:, cols(z)], osend.at[i], orecv.at[z], here.chip(i, y, x)
        )

    def fold(op, value):
        total = value[:, :VD]
        for j in range(1, chunk // VD):
            total = op(total, value[:, j * VD : (j + 1) * VD])
        return total

    def block(i, carry):
        query = (qb[i].astype(jnp.float32) * HD ** (-0.5)).astype(jnp.bfloat16)
        zero = jnp.zeros_like(query)
        both = jnp.concatenate(
            (jnp.where(lane < HD, query, zero), jnp.where(lane < HD, zero, query)), axis=0
        )

        def scores_of(c):
            return lax.dot_general(
                both, kb[span(c, chunk), :], (((1,), (1,)), ((), ())),
                preferred_element_type=jnp.float32,
            )

        def score(c, peak):
            scores = scores_of(c)
            sb[c] = scores
            return jnp.maximum(peak, fold(jnp.maximum, scores))

        peak = lax.fori_loop(0, i, score, jnp.full((2 * rows, VD), neg_fill, jnp.float32))
        scores = scores_of(i)
        row = lax.broadcasted_iota(jnp.int32, scores.shape, 0)
        row = jnp.where(row < rows, row, row - rows)
        col = lax.broadcasted_iota(jnp.int32, scores.shape, 1)
        scores = jnp.where(col <= w * rows + row, scores, neg_fill)
        sb[i] = scores
        peak = jnp.maximum(peak, fold(jnp.maximum, scores))
        top = jnp.max(peak, axis=-1, keepdims=True)

        def weigh(c, state):
            total, acc = state
            exp_scores = jnp.exp(sb[c] - top)
            total = total + fold(jnp.add, exp_scores)
            acc = acc + jnp.dot(
                exp_scores.astype(jnp.bfloat16), vb[span(c, chunk), :],
                preferred_element_type=jnp.float32,
            )
            return total, acc

        blank = jnp.zeros((2 * rows, VD), jnp.float32)
        total, acc = lax.fori_loop(0, i + 1, weigh, (blank, blank))
        mean_v = acc / jnp.sum(total, axis=-1, keepdims=True)
        diff = mean_v[:rows] - weight * mean_v[rows:]
        inv = lax.rsqrt(jnp.mean(diff * diff, axis=-1, keepdims=True) + eps)
        result = (diff * inv * gain_row * 0.8).astype(jnp.bfloat16)

        @pl.when(i != z)
        def _():
            ob[i] = result
            answer(i).start()

        @pl.when(i == z)
        def _():
            att[:, cols(z)] = result

        @pl.when(i == 0)
        def _():
            pass_on(0, 1)

        @pl.when(i > 0)
        def _():
            pass_on(jnp.maximum(i, 1), 0)

        return carry

    lax.fori_loop(0, layers, block, 0)
    for a in range(1, layers):
        for copy in weights(a, 1):
            copy.start()

    def answered(a, carry):
        h = here.behind(a)
        to_sp(ob.at[0], att.at[:, cols(h)], osend.at[0], orecv.at[h], me).wait_recv()
        return carry

    lax.fori_loop(1, layers, answered, 0)
    mine = span(t, half)
    theirs = span(1 - t, half)
    pbuf[...] = jnp.dot(att[theirs, :], ow[...], preferred_element_type=jnp.float32).astype(
        jnp.bfloat16
    )
    swap = to_tp(pbuf, prbuf, tsem.at[0], tsem.at[1], 1 - t)
    swap.start()
    own = jnp.dot(att[mine, :], ow[...], preferred_element_type=jnp.float32).astype(jnp.bfloat16)
    swap.wait()
    proj = (own.astype(jnp.float32) + prbuf[...].astype(jnp.float32)).astype(jnp.bfloat16)
    mid_v = (res[...].astype(jnp.float32) + proj.astype(jnp.float32)).astype(jnp.bfloat16)
    mid[...] = mid_v
    mid_f = mid_v.astype(jnp.float32)
    inv = lax.rsqrt(jnp.mean(mid_f * mid_f, axis=-1, keepdims=True) + eps)
    normed[...] = (mid_f * inv * ngain[...]).astype(jnp.bfloat16)

    def late(a, carry):
        pass_on(a, 1)
        return carry

    lax.fori_loop(1, layers, late, 0)

    def drain(a, carry):
        for b in range(2):
            for copy in across_x(a, b):
                copy.wait_recv()
                copy.wait_send()
        for copy in in_plane(a) + corner(a):
            copy.wait_send()

        @pl.when(a != z)
        def _():
            answer(a).wait_send()

        @pl.when(a > 0)
        def _():
            for copy in along_z(a) + weights(a, 0):
                copy.wait_send()

        for copy in weights(a, 1):
            copy.wait_send()
        return carry

    lax.fori_loop(0, layers, drain, 0)


def ffn_kernel(
    n, normed, mid, wu, wg, wd, cw, cb, out,
    buf, up, gate, tails, halo, hid, pb, pr, sb, rb, zb, cbuf,
    send, recv, fsend, frecv, hsend, hrecv,
    xsend, xrecv, ysend, yrecv, zsend, zrecv,
):
    here = Place(n)
    me, t, z, y, x = here.me, here.t, here.z, here.y, here.x
    layers = here.layers
    groups = n // 2
    half = mid.shape[0]
    rows = 2 * half
    rim = tails.shape[1]
    taps = cw.shape[0]
    wide = wu.shape[1]
    tiles = cw.shape[1] // VD
    mine = span(t, half)
    theirs = span(1 - t, half)
    greet(n, me, t)
    buf[0, mine, :] = normed[...]
    halo[0] = jnp.zeros(halo.shape[1:], jnp.bfloat16)

    def column(a):
        dest = here.chip(here.ahead(a), y, x)
        return to_sp(buf.at[0, mine], buf.at[a * 2, mine], send.at[a * 2], recv.at[a * 2], dest)

    def spread(a):
        return to_sp(
            buf.at[a * 2, mine], buf.at[a * 2 + 1, mine],
            send.at[a * 2 + 1], recv.at[a * 2 + 1], here.yn,
        )

    def forward(slot):
        return to_tp(
            buf.at[slot, mine], buf.at[slot, mine], fsend.at[slot], frecv.at[slot], 1 - t
        )

    def arrived(slot):
        return to_tp(
            buf.at[slot, theirs], buf.at[slot, theirs], fsend.at[slot], frecv.at[slot], 1 - t
        )

    def tail(j):
        return to_sp(tails.at[j], halo.at[j + 1], hsend.at[j], hrecv.at[j], here.xn)

    def compute(a, b):
        slot = a * 2 + b
        arrived(slot).wait_recv()
        j = here.behind(a) * 2 + lax.rem(y + b, 2)
        rows_in = buf[slot]
        up_v = jnp.dot(rows_in, wu[...], preferred_element_type=jnp.float32).astype(jnp.bfloat16)
        up[span(j, rows), :] = up_v
        tails[j] = up_v[rows - rim :]
        tail(j).start()
        gate[span(j, rows), :] = jnp.dot(
            rows_in, wg[...], preferred_element_type=jnp.float32
        ).astype(jnp.bfloat16)

    for a in range(1, layers):
        column(a).start()
    spread(0).start()
    forward(0).start()

    def stage(a, carry):
        @pl.when(a + 1 < layers)
        def _():
            column(a + 1).wait_recv()
            spread(a + 1).start()
            forward(2 * (a + 1)).start()

        compute(a, 0)
        spread(a).wait_recv()
        forward(2 * a + 1).start()
        compute(a, 1)
        return carry

    lax.fori_loop(0, layers, stage, 0)

    group = z * 2 + y
    start = first_tile(group, tiles, groups)
    before = first_tile(group - 1, tiles, groups) + wide // VD
    twice = jnp.where(group > 0, jnp.maximum(before - start, 0), 0) * VD
    part = pl.ds(pl.multiple_of(start * VD, VD), wide)

    def place(i):
        return lax.rem(i // 2 + 1, layers), lax.rem(lax.rem(i, 2) + 1, 2)

    def swap(slot):
        return to_tp(pb.at[slot], pr.at[slot], xsend.at[slot], xrecv.at[slot], 1 - t)

    def across(a):
        return to_sp(sb.at[a * 2 + 1], rb.at[a], ysend.at[a], yrecv.at[a], here.yn)

    def upright(a):
        dest = here.chip(here.ahead(a), y, x)
        return to_sp(zb.at[a], cbuf.at[a], zsend.at[a], zrecv.at[a], dest)

    def hidden(j):
        prior = jnp.where(x == 1, j, j - 1)

        @pl.when(prior >= 0)
        def _():
            tail(jnp.maximum(prior, 0)).wait_recv()

        edge = halo[prior + 1].astype(jnp.float32)
        now = up[span(j, rows), :].astype(jnp.float32)
        row = lax.broadcasted_iota(jnp.int32, now.shape, 0)
        conv = cb[:, part] + cw[pl.ds(taps - 1, 1), part] * now
        for back in range(1, taps):
            moved = pltpu.roll(now, back, 0)
            for r in range(back):
                moved = jnp.where(row == r, edge[rim - back + r][None, :], moved)
            conv = conv + cw[pl.ds(taps - 1 - back, 1), part] * moved
        act = conv / (1.0 + jnp.exp(-conv)) * gate[span(j, rows), :].astype(jnp.float32)
        lane = lax.broadcasted_iota(jnp.int32, act.shape, 1)
        hid[...] = jnp.where(lane < twice, 0.0, act).astype(jnp.bfloat16)

    def product(i):
        a, b = place(i)
        slot = a * 2 + b
        hidden(here.ahead(a) * 2 + lax.rem(y + b, 2))
        pb[slot] = jnp.dot(hid[theirs, :], wd[...], preferred_element_type=jnp.float32).astype(
            jnp.bfloat16
        )
        swap(slot).start()
        sb[slot] = jnp.dot(hid[mine, :], wd[...], preferred_element_type=jnp.float32).astype(
            jnp.bfloat16
        )

    def combine(i):
        a, b = place(i)
        slot = a * 2 + b
        swap(slot).wait_recv()
        sb[slot] = (sb[slot].astype(jnp.float32) + pr[slot].astype(jnp.float32)).astype(
            jnp.bfloat16
        )

        @pl.when(b != 0)
        def _():
            across(a).start()

    def plane_sum(a):
        across(a).wait_recv()
        return sb[a * 2].astype(jnp.float32) + rb[a].astype(jnp.float32)

    product(0)

    def step(i, carry):
        product(i)
        combine(i - 1)

        @pl.when(jnp.logical_and(lax.rem(i, 2) == 1, i >= 2))
        def _():
            a = i // 2
            zb[a] = plane_sum(a).astype(jnp.bfloat16)
            upright(a).start()

        return carry

    lax.fori_loop(1, groups, step, 0)
    combine(groups - 1)
    acc = plane_sum(0)
    for a in range(1, layers):
        upright(a).wait_recv()
        acc = acc + cbuf[a].astype(jnp.float32)
    ffn = acc.astype(jnp.bfloat16).astype(jnp.float32)
    out[...] = (mid[...].astype(jnp.float32) + ffn).astype(jnp.bfloat16)

    @pl.when(x == 0)
    def _():
        tail(groups - 1).wait_recv()

    def drain(a, carry):
        spread(a).wait_send()
        across(a).wait_send()
        for b in range(2):
            forward(a * 2 + b).wait_send()
            swap(a * 2 + b).wait_send()
            tail(a * 2 + b).wait_send()

        @pl.when(a > 0)
        def _():
            column(a).wait_send()
            upright(a).wait_send()

        return carry

    lax.fori_loop(0, layers, drain, 0)


def vm(count):
    return [pl.BlockSpec(memory_space=pltpu.VMEM)] * count


def params(cid):
    return pltpu.CompilerParams(
        collective_id=cid, has_side_effects=True, vmem_limit_bytes=VMEM_LIMIT
    )


def moving_rows(
    n,
    residual,
    queries,
    key_pairs,
    values,
    second_weight,
    head_gain,
    out_weight,
    norm_gain,
    up_weight,
    gate_weight,
    conv_weight,
    conv_bias,
    down_weight,
):
    rows, width = queries.shape
    half, model = residual.shape
    heads = second_weight.shape[0]
    depth, ff_local = up_weight.shape
    layers = n // 4
    groups = n // 2
    wide = tile_count(ff_local // VD, groups) * VD
    bf = jnp.bfloat16
    f32 = jnp.float32
    dma = pltpu.SemaphoreType.DMA
    shape = jax.ShapeDtypeStruct
    tall = shape((n * depth, wide), bf)
    mid, normed, wu, wg, wd = pl.pallas_call(
        functools.partial(attention_kernel, n),
        out_shape=(
            shape((half, model), bf), shape((half, model), bf),
            tall, tall, shape((wide, n * depth), bf),
        ),
        in_specs=vm(3) + [pl.BlockSpec(memory_space=pltpu.SMEM)] + vm(7),
        out_specs=tuple(vm(5)),
        scratch_shapes=[
            pltpu.VMEM((layers, rows, VD), bf),
            pltpu.VMEM((n * rows, VD), bf),
            pltpu.VMEM((n * rows, VD), bf),
            pltpu.VMEM((layers, rows, VD), bf),
            pltpu.VMEM((layers, 2 * rows, 4 * rows), f32),
            pltpu.VMEM((rows, width), bf),
            pltpu.VMEM((half, model), bf),
            pltpu.VMEM((half, model), bf),
            dma((3, layers)), dma((3, layers)),
            dma((6, layers)), dma((6, layers)),
            dma((layers,)), dma((layers,)), dma((2,)),
            dma((3, groups)), dma((3, groups)), dma((3, groups)), dma((3, groups)),
        ],
        compiler_params=params(0),
        name="attend_rows",
    )(
        queries, key_pairs, values, second_weight, head_gain.reshape(heads, VD),
        out_weight, residual, norm_gain[None, :], up_weight, gate_weight, down_weight,
    )
    block = pltpu.VMEM((groups, half, model), bf)
    few = pltpu.VMEM((layers, half, model), bf)
    rim = 16
    return pl.pallas_call(
        functools.partial(ffn_kernel, n),
        out_shape=shape((half, model), bf),
        in_specs=vm(7),
        out_specs=vm(1)[0],
        scratch_shapes=[
            pltpu.VMEM((groups, rows, model), bf),
            pltpu.VMEM((groups * rows, wide), bf),
            pltpu.VMEM((groups * rows, wide), bf),
            pltpu.VMEM((groups, rim, wide), bf),
            pltpu.VMEM((groups + 1, rim, wide), bf),
            pltpu.VMEM((rows, wide), bf),
            block, block, block, few, few, few,
        ]
        + [dma((groups,))] * 8
        + [dma((layers,))] * 4,
        compiler_params=params(1),
        name="ffn_rows",
    )(normed, mid, wu, wg, wd, conv_weight, conv_bias[None, :])


def choose(n_sp, n_tp):
    def body(residual, queries, *rest):
        up_weight = rest[6]
        moves_rows = (
            n_tp == 2
            and n_sp % 4 == 0
            and rest[2].shape[0] == n_sp // 4
            and up_weight.shape[1] % VD == 0
            and up_weight.shape[1] // VD >= n_sp // 2
            and queries.shape[0] % 32 == 0
            and up_weight.shape[0] % VD == 0
            and rest[8].shape[0] <= 16
        )
        if moves_rows:
            return moving_rows(n_sp, residual, queries, *rest)
        return local(residual, queries, *rest)

    return body


def solution(mesh):
    return jax.shard_map(
        choose(mesh.shape["sp"], mesh.shape["tp"]),
        mesh=mesh,
        in_specs=(
            P(("sp", "tp"), None),
            P("sp", "tp"),
            P("sp", "tp"),
            P("sp", "tp"),
            P("tp"),
            P("tp"),
            P("tp", None),
            P(),
            P("sp", "tp"),
            P("sp", "tp"),
            P(None, "tp"),
            P("tp"),
            P("tp", "sp"),
        ),
        out_specs=P(("sp", "tp"), None),
        check_vma=False,
    )
```

```python
import functools

import jax
import jax.numpy as jnp
from jax import lax
from jax.experimental import pallas as pl
from jax.experimental.pallas import tpu as pltpu
from jax.sharding import PartitionSpec as P

MESH = pl.DeviceIdType.MESH
VMEM_LIMIT = 60 * 1024 * 1024

HD = 64
VD = 128


eps = 1e-05
neg_fill = -1e30


def from_behind(value, axis, steps):
    count = lax.axis_size(axis)
    leading, last = (max(0, -steps), min(count, count - steps))
    return lax.ppermute(value, axis, [(source, source + steps) for source in range(leading, last)])


def normalize(rows_in, gain):
    values_f = rows_in.astype(jnp.float32)
    scale_inv = lax.rsqrt(jnp.mean(values_f * values_f, axis=-1, keepdims=True) + eps)
    return (values_f * scale_inv * gain).astype(jnp.bfloat16)


def attend(queries, key_pairs, values, second_weight, head_gain):
    tok_rows = queries.shape[0]
    head_count = second_weight.shape[0]
    sp_index = lax.axis_index("sp")
    query = queries.reshape(tok_rows, head_count, 2, HD)
    query_pos = sp_index * tok_rows + jnp.arange(tok_rows)
    last_query = (sp_index + 1) * tok_rows
    initial = (
        jnp.full((head_count, 2, tok_rows), neg_fill, jnp.float32),
        jnp.zeros((head_count, 2, tok_rows), jnp.float32),
        jnp.zeros((head_count, 2, tok_rows, VD), jnp.float32),
    )
    key_piece = lax.all_gather(key_pairs, "sp", axis=0, tiled=True)
    value_piece = lax.all_gather(values, "sp", axis=0, tiled=True)
    piece_len = key_piece.shape[0]

    def compute(state_in):
        maxima, totals, weighted = state_in
        key_rows = key_piece.reshape(piece_len, head_count, 2, HD)
        value_rows = value_piece.reshape(piece_len, head_count, VD)
        scores = jnp.einsum(
            "qhmd,khmd->hmqk", query, key_rows, preferred_element_type=jnp.float32
        ) * HD ** (-0.5)
        visible = jnp.arange(piece_len)[None, :] <= query_pos[:, None]
        scores = jnp.where(visible, scores, neg_fill)
        new_max = jnp.maximum(maxima, jnp.max(scores, axis=-1))
        exp_scores = jnp.where(visible, jnp.exp(scores - new_max[..., None]), jnp.float32(0.0))
        totals = jnp.sum(exp_scores, axis=-1)
        weighted = jnp.einsum(
            "hmqk,khe->hmqe",
            exp_scores.astype(jnp.bfloat16),
            value_rows,
            preferred_element_type=jnp.float32,
        )
        return (new_max, totals, weighted)

    def keep_state(state_in):
        return state_in

    maxima, totals, weighted = lax.cond(jnp.int32(0) < last_query, compute, keep_state, initial)
    diff = (
        weighted[:, 0] / totals[:, 0, :, None]
        - second_weight[:, None, None] * weighted[:, 1] / totals[:, 1, :, None]
    )
    diff = jnp.transpose(diff, (1, 0, 2))
    scale_inv = lax.rsqrt(jnp.mean(diff * diff, axis=-1, keepdims=True) + eps)
    attended = (
        (diff * scale_inv * head_gain.reshape(head_count, VD) * 0.8)
        .reshape(tok_rows, head_count * VD)
        .astype(jnp.bfloat16)
    )
    return attended


def local(
    residual,
    queries,
    key_pairs,
    values,
    second_weight,
    head_gain,
    out_weight,
    norm_gain,
    up_weight,
    gate_weight,
    conv_weight,
    conv_bias,
    down_weight,
):
    tok_rows = queries.shape[0]
    ff_local = up_weight.shape[1]
    attended = attend(queries, key_pairs, values, second_weight, head_gain)
    proj = lax.psum_scatter(
        jnp.dot(attended, out_weight, preferred_element_type=jnp.float32).astype(jnp.bfloat16),
        "tp",
        scatter_dimension=0,
        tiled=True,
    )
    mid = (residual.astype(jnp.float32) + proj.astype(jnp.float32)).astype(jnp.bfloat16)
    normed_all = lax.all_gather(normalize(mid, norm_gain), "tp", axis=0, tiled=True)
    up_sum = jnp.dot(
        normed_all,
        lax.all_gather(up_weight, "sp", axis=0, tiled=True),
        preferred_element_type=jnp.float32,
    )
    gate_sum = jnp.dot(
        normed_all,
        lax.all_gather(gate_weight, "sp", axis=0, tiled=True),
        preferred_element_type=jnp.float32,
    )
    up_proj = up_sum.astype(jnp.bfloat16)
    gate_proj = gate_sum.astype(jnp.bfloat16)
    taps = conv_weight.shape[0]
    rim_rows = from_behind(up_proj[tok_rows - (taps - 1) :], "sp", 1)
    extended = jnp.concatenate((rim_rows, up_proj), axis=0)
    conv_out = jnp.zeros((tok_rows, ff_local), jnp.float32) + conv_bias[None, :]
    for tap in range(taps):
        conv_out = conv_out + conv_weight[tap][None, :] * extended[tap : tap + tok_rows].astype(
            jnp.float32
        )
    hidden = (jax.nn.silu(conv_out) * gate_proj.astype(jnp.float32)).astype(jnp.bfloat16)
    down_all = lax.all_gather(down_weight, "sp", axis=1, tiled=True)
    ffn_out = lax.psum_scatter(
        jnp.dot(hidden, down_all, preferred_element_type=jnp.float32).astype(jnp.bfloat16),
        "tp",
        scatter_dimension=0,
        tiled=True,
    )
    return (mid.astype(jnp.float32) + ffn_out.astype(jnp.float32)).astype(jnp.bfloat16)


def greet(n, me, t):
    barrier = pltpu.get_barrier_semaphore()

    def signal(k, carry):
        pl.semaphore_signal(
            barrier, inc=1, device_id={"sp": lax.rem(me + k, n)}, device_id_type=MESH
        )
        return carry

    lax.fori_loop(1, n, signal, 0)
    pl.semaphore_signal(barrier, inc=1, device_id={"tp": 1 - t}, device_id_type=MESH)
    pl.semaphore_wait(barrier, n)


def to_sp(src, dst, send, recv, dest):
    return pltpu.make_async_remote_copy(
        src_ref=src, dst_ref=dst, send_sem=send, recv_sem=recv,
        device_id={"sp": dest}, device_id_type=MESH,
    )


def to_tp(src, dst, send, recv, dest):
    return pltpu.make_async_remote_copy(
        src_ref=src, dst_ref=dst, send_sem=send, recv_sem=recv,
        device_id={"tp": dest}, device_id_type=MESH,
    )


def span(index, size):
    return pl.ds(pl.multiple_of(index * size, size), size)


def first_tile(group, tiles, groups):
    return group * tiles // groups


def tile_count(tiles, groups):
    return -(-tiles // groups)


class Place:
    def __init__(self, n):
        self.n = n
        self.layers = n // 4
        self.me = lax.axis_index("sp")
        self.t = lax.axis_index("tp")
        self.z = self.me // 4
        self.w = lax.rem(self.me, 4)
        self.y = self.w // 2
        self.x = lax.rem(self.w, 2)
        self.xn = self.z * 4 + self.y * 2 + (1 - self.x)
        self.yn = self.z * 4 + (1 - self.y) * 2 + self.x

    def ahead(self, a):
        return lax.rem(self.z + a, self.layers)

    def behind(self, a):
        return lax.rem(self.z - a + self.layers, self.layers)

    def chip(self, z, y, x):
        return z * 4 + y * 2 + x


def layer_kernel(
    n, q, k, v, sw, gain, ow, res, ngain, uw, gw, dw, cw, cb,
    out,
    wu, wg, wd, mid, qb, kb, vb, ob, sb, att, pbuf, prbuf,
    buf, up, gate, tails, halo, hid, pb, pr, kept, rb, zb, cbuf,
    zsend, zrecv, psend, precv, osend, orecv, tsem, wsend, wrecv, fsend, frecv,
    usend, dsend, lrecv, rsend, rrecv, csend, crecv, hsend, hrecv,
    xsend, xrecv, ysend, yrecv, ssend, srecv,
):
    here = Place(n)
    me, t, z, w, y, x = here.me, here.t, here.z, here.w, here.y, here.x
    layers = here.layers
    rows = q.shape[0]
    half = rows // 2
    depth = uw.shape[0]
    groups = n // 2
    tiles = uw.shape[1] // VD
    wide = wu.shape[1]
    chunk = 4 * rows
    greet(n, me, t)

    def cols(h):
        return span(h, VD)

    def along_z(a):
        zz = here.ahead(a)
        dest = here.chip(zz, y, x)
        return (
            to_sp(k.at[:, cols(zz)], kb.at[span(me, rows)], zsend.at[0, a], zrecv.at[0, a], dest),
            to_sp(v.at[:, cols(zz)], vb.at[span(me, rows)], zsend.at[1, a], zrecv.at[1, a], dest),
            to_sp(q.at[:, cols(zz)], qb.at[z], zsend.at[2, a], zrecv.at[2, a], dest),
        )

    def in_plane(a):
        own = span(here.behind(a) * 4 + w, rows)
        return (
            to_sp(kb.at[own], kb.at[own], psend.at[0, a], precv.at[0, a], here.xn),
            to_sp(vb.at[own], vb.at[own], psend.at[1, a], precv.at[1, a], here.yn),
            to_sp(vb.at[own], vb.at[own], psend.at[2, a], precv.at[2, a], here.xn),
            to_sp(kb.at[own], kb.at[own], psend.at[3, a], precv.at[3, a], here.yn),
        )

    def corner(a):
        from_x = span(here.chip(here.behind(a), y, 1 - x), rows)
        from_y = span(here.chip(here.behind(a), 1 - y, x), rows)
        return (
            to_sp(kb.at[from_x], kb.at[from_x], psend.at[4, a], precv.at[4, a], here.yn),
            to_sp(vb.at[from_y], vb.at[from_y], psend.at[5, a], precv.at[5, a], here.xn),
        )

    def weights(a, b):
        slot = a * 2 + b
        zz = here.ahead(a)
        yy = lax.rem(y + b, 2)
        dest = here.chip(zz, yy, x)
        first = pl.multiple_of(first_tile(zz * 2 + yy, tiles, groups) * VD, VD)
        part = pl.ds(first, wide)
        mine = span(me, depth)
        return (
            to_sp(uw.at[:, part], wu.at[mine], wsend.at[0, slot], wrecv.at[0, slot], dest),
            to_sp(gw.at[:, part], wg.at[mine], wsend.at[1, slot], wrecv.at[1, slot], dest),
            to_sp(dw.at[part], wd.at[:, mine], wsend.at[2, slot], wrecv.at[2, slot], dest),
        )

    def across_x(a, b):
        slot = a * 2 + b
        got = span(here.chip(here.behind(a), lax.rem(y + b, 2), x), depth)
        return (
            to_sp(wu.at[got], wu.at[got], fsend.at[0, slot], frecv.at[0, slot], here.xn),
            to_sp(wg.at[got], wg.at[got], fsend.at[1, slot], frecv.at[1, slot], here.xn),
            to_sp(
                wd.at[:, got], wd.at[:, got], fsend.at[2, slot], frecv.at[2, slot], here.xn
            ),
        )

    def pass_on(a, b):
        for copy in weights(a, b):
            copy.wait_recv()
        for copy in across_x(a, b):
            copy.start()

    for a in range(1, layers):
        for copy in along_z(a):
            copy.start()
    kb[span(me, rows), :] = k[:, cols(z)]
    vb[span(me, rows), :] = v[:, cols(z)]
    qb[z] = q[:, cols(z)]
    for copy in in_plane(0):
        copy.start()
    for a in range(1, layers):
        for copy in weights(a, 0):
            copy.start()
    for copy in weights(0, 1):
        copy.start()
    own_first = pl.multiple_of(first_tile(z * 2 + y, tiles, groups) * VD, VD)
    own_part = pl.ds(own_first, wide)
    wu[span(me, depth), :] = uw[:, own_part]
    wg[span(me, depth), :] = gw[:, own_part]
    wd[:, span(me, depth)] = dw[own_part, :]

    def corner_stage(a):
        in_plane(a)[0].wait_recv()
        corner(a)[0].start()
        in_plane(a)[1].wait_recv()
        corner(a)[1].start()

    def stage(a, carry):
        copies = along_z(a)
        copies[0].wait_recv()
        copies[1].wait_recv()
        for copy in in_plane(a):
            copy.start()
        corner_stage(a - 1)
        return carry

    lax.fori_loop(1, layers, stage, 0)
    corner_stage(layers - 1)
    for copy in across_x(0, 0):
        copy.start()

    def settle(a, carry):
        in_plane(a)[2].wait_recv()
        in_plane(a)[3].wait_recv()
        corner(a)[0].wait_recv()
        corner(a)[1].wait_recv()
        return carry

    lax.fori_loop(0, layers, settle, 0)
    for a in range(1, layers):
        along_z(a)[2].wait_recv()

    weight = sw[z]
    gain_row = gain[pl.ds(z, 1), :]
    lane = lax.broadcasted_iota(jnp.int32, (rows, VD), 1)

    def answer(i):
        return to_sp(
            ob.at[i], att.at[:, cols(z)], osend.at[i], orecv.at[z], here.chip(i, y, x)
        )

    def fold(op, value):
        total = value[:, :VD]
        for j in range(1, chunk // VD):
            total = op(total, value[:, j * VD : (j + 1) * VD])
        return total

    def block(i, carry):
        query = (qb[i].astype(jnp.float32) * HD ** (-0.5)).astype(jnp.bfloat16)
        zero = jnp.zeros_like(query)
        both = jnp.concatenate(
            (jnp.where(lane < HD, query, zero), jnp.where(lane < HD, zero, query)), axis=0
        )

        def scores_of(c):
            return lax.dot_general(
                both, kb[span(c, chunk), :], (((1,), (1,)), ((), ())),
                preferred_element_type=jnp.float32,
            )

        def score(c, peak):
            scores = scores_of(c)
            sb[c] = scores
            return jnp.maximum(peak, fold(jnp.maximum, scores))

        peak = lax.fori_loop(0, i, score, jnp.full((2 * rows, VD), neg_fill, jnp.float32))
        scores = scores_of(i)
        row = lax.broadcasted_iota(jnp.int32, scores.shape, 0)
        row = jnp.where(row < rows, row, row - rows)
        col = lax.broadcasted_iota(jnp.int32, scores.shape, 1)
        scores = jnp.where(col <= w * rows + row, scores, neg_fill)
        sb[i] = scores
        peak = jnp.maximum(peak, fold(jnp.maximum, scores))
        top = jnp.max(peak, axis=-1, keepdims=True)

        def weigh(c, state):
            total, acc = state
            exp_scores = jnp.exp(sb[c] - top)
            total = total + fold(jnp.add, exp_scores)
            acc = acc + jnp.dot(
                exp_scores.astype(jnp.bfloat16), vb[span(c, chunk), :],
                preferred_element_type=jnp.float32,
            )
            return total, acc

        blank = jnp.zeros((2 * rows, VD), jnp.float32)
        total, acc = lax.fori_loop(0, i + 1, weigh, (blank, blank))
        mean_v = acc / jnp.sum(total, axis=-1, keepdims=True)
        diff = mean_v[:rows] - weight * mean_v[rows:]
        inv = lax.rsqrt(jnp.mean(diff * diff, axis=-1, keepdims=True) + eps)
        result = (diff * inv * gain_row * 0.8).astype(jnp.bfloat16)

        @pl.when(i != z)
        def _():
            ob[i] = result
            answer(i).start()

        @pl.when(i == z)
        def _():
            att[:, cols(z)] = result

        @pl.when(i == 0)
        def _():
            pass_on(0, 1)

        @pl.when(i > 0)
        def _():
            pass_on(jnp.maximum(i, 1), 0)

        return carry

    lax.fori_loop(0, layers, block, 0)
    for a in range(1, layers):
        for copy in weights(a, 1):
            copy.start()

    def answered(a, carry):
        h = here.behind(a)
        to_sp(ob.at[0], att.at[:, cols(h)], osend.at[0], orecv.at[h], me).wait_recv()
        return carry

    lax.fori_loop(1, layers, answered, 0)
    mine = span(t, half)
    theirs = span(1 - t, half)
    pbuf[...] = jnp.dot(att[theirs, :], ow[...], preferred_element_type=jnp.float32).astype(
        jnp.bfloat16
    )
    swap = to_tp(pbuf, prbuf, tsem.at[0], tsem.at[1], 1 - t)
    swap.start()
    own = jnp.dot(att[mine, :], ow[...], preferred_element_type=jnp.float32).astype(jnp.bfloat16)
    swap.wait()
    proj = (own.astype(jnp.float32) + prbuf[...].astype(jnp.float32)).astype(jnp.bfloat16)
    mid_v = (res[...].astype(jnp.float32) + proj.astype(jnp.float32)).astype(jnp.bfloat16)
    mid[...] = mid_v
    mid_f = mid_v.astype(jnp.float32)
    inv = lax.rsqrt(jnp.mean(mid_f * mid_f, axis=-1, keepdims=True) + eps)
    home = z * 2 + y
    buf[home, mine, :] = (mid_f * inv * ngain[...]).astype(jnp.bfloat16)
    halo[0] = jnp.zeros(halo.shape[1:], jnp.bfloat16)

    rim = tails.shape[1]
    taps = cw.shape[0]

    def line_up(zz):
        slot = zz * 2 + y
        dest = here.chip(jnp.minimum(z + 1, layers - 1), y, x)
        return to_sp(buf.at[slot, mine], buf.at[slot, mine], usend.at[zz], lrecv.at[zz], dest)

    def line_down(zz):
        slot = zz * 2 + y
        dest = here.chip(jnp.maximum(z - 1, 0), y, x)
        return to_sp(buf.at[slot, mine], buf.at[slot, mine], dsend.at[zz], lrecv.at[zz], dest)

    def spread(zz):
        slot = zz * 2 + y
        return to_sp(
            buf.at[slot, mine], buf.at[slot, mine], rsend.at[zz], rrecv.at[zz], here.yn
        )

    def spread_in(zz):
        slot = zz * 2 + 1 - y
        return to_sp(
            buf.at[slot, mine], buf.at[slot, mine], rsend.at[zz], rrecv.at[zz], here.yn
        )

    def forward(slot):
        return to_tp(
            buf.at[slot, mine], buf.at[slot, mine], csend.at[slot], crecv.at[slot], 1 - t
        )

    def arrived(slot):
        return to_tp(
            buf.at[slot, theirs], buf.at[slot, theirs], csend.at[slot], crecv.at[slot], 1 - t
        )

    def tail(j):
        return to_sp(tails.at[j], halo.at[j + 1], hsend.at[j], hrecv.at[j], here.xn)

    def compute(j):
        arrived(j).wait_recv()
        rows_in = buf[j]
        up_v = jnp.dot(rows_in, wu[...], preferred_element_type=jnp.float32).astype(jnp.bfloat16)
        up[span(j, rows), :] = up_v
        tails[j] = up_v[rows - rim :]
        tail(j).start()
        gate[span(j, rows), :] = jnp.dot(
            rows_in, wg[...], preferred_element_type=jnp.float32
        ).astype(jnp.bfloat16)

    @pl.when(z + 1 < layers)
    def _():
        line_up(z).start()

    @pl.when(z > 0)
    def _():
        line_down(z).start()

    spread(z).start()
    forward(home).start()

    def late(a, carry):
        pass_on(a, 1)
        return carry

    lax.fori_loop(1, layers, late, 0)

    def line_step(d):
        low, high = z - d, z + d

        @pl.when(low >= 0)
        def _():
            line_up(low).wait_recv()

            @pl.when(z + 1 < layers)
            def _():
                line_up(low).start()

            spread(low).start()
            forward(low * 2 + y).start()

        @pl.when(high < layers)
        def _():
            line_down(high).wait_recv()

            @pl.when(z > 0)
            def _():
                line_down(high).start()

            spread(high).start()
            forward(high * 2 + y).start()

    line_step(1)

    def crossed(a, carry):
        for b in range(2):
            for copy in across_x(a, b):
                copy.wait_recv()
        return carry

    lax.fori_loop(0, layers, crossed, 0)

    def stage_rows(d, carry):
        @pl.when(jnp.logical_and(d > 0, d + 1 < layers))
        def _():
            line_step(d + 1)

        low, high = z - d, z + d
        has_low = low >= 0
        has_high = jnp.logical_and(high < layers, d > 0)

        @pl.when(has_low)
        def _():
            compute(low * 2 + y)
            spread_in(low).wait_recv()
            forward(low * 2 + 1 - y).start()

        @pl.when(has_high)
        def _():
            compute(high * 2 + y)
            spread_in(high).wait_recv()
            forward(high * 2 + 1 - y).start()

        @pl.when(has_low)
        def _():
            compute(low * 2 + 1 - y)

        @pl.when(has_high)
        def _():
            compute(high * 2 + 1 - y)

        return carry

    lax.fori_loop(0, layers, stage_rows, 0)

    start = first_tile(home, tiles, groups)
    before = first_tile(home - 1, tiles, groups) + wide // VD
    twice = jnp.where(home > 0, jnp.maximum(before - start, 0), 0) * VD
    part = pl.ds(pl.multiple_of(start * VD, VD), wide)
    bias = jnp.concatenate([cb[pl.ds(start + j, 1), :] for j in range(wide // VD)], axis=1)

    below, above = z, layers - 1 - z

    def order(i):
        lead = jnp.abs(above - below)
        k = i - lead
        more_above = above >= below
        far = jnp.where(more_above, layers - 1 - i, i)
        near_even = jnp.where(more_above, k // 2, layers - 1 - k // 2)
        near_odd = jnp.where(more_above, layers - 1 - lead - k // 2, lead + k // 2)
        near = jnp.where(lax.rem(k + layers * 2, 2) == 0, near_even, near_odd)
        pick = jnp.where(i < lead, far, near)
        return jnp.where(i >= layers - 1, z, pick)

    def swap_sums(slot):
        return to_tp(pb.at[slot], pr.at[slot], xsend.at[slot], xrecv.at[slot], 1 - t)

    def across(zz):
        return to_sp(kept.at[zz * 2 + 1 - y], rb.at[zz], ysend.at[zz], yrecv.at[zz], here.yn)

    def chain(zz, landing, dest):
        return to_sp(zb.at[zz], cbuf.at[landing], ssend.at[zz], srecv.at[landing], dest)

    def hidden(j):
        prior = jnp.where(x == 1, j, j - 1)

        @pl.when(prior >= 0)
        def _():
            tail(jnp.maximum(prior, 0)).wait_recv()

        edge = halo[prior + 1].astype(jnp.float32)
        now = up[span(j, rows), :].astype(jnp.float32)
        row = lax.broadcasted_iota(jnp.int32, now.shape, 0)
        conv = bias + cw[pl.ds(taps - 1, 1), part] * now
        for back in range(1, taps):
            moved = pltpu.roll(now, back, 0)
            for r in range(back):
                moved = jnp.where(row == r, edge[rim - back + r][None, :], moved)
            conv = conv + cw[pl.ds(taps - 1 - back, 1), part] * moved
        act = conv / (1.0 + jnp.exp(-conv)) * gate[span(j, rows), :].astype(jnp.float32)
        lane_of = lax.broadcasted_iota(jnp.int32, act.shape, 1)
        hid[...] = jnp.where(lane_of < twice, 0.0, act).astype(jnp.bfloat16)

    def slot_of(i):
        side = jnp.where(i < layers, 1 - y, y)
        return order(lax.rem(i, layers)) * 2 + side

    def product(i):
        slot = slot_of(i)
        hidden(slot)
        pb[slot] = jnp.dot(hid[theirs, :], wd[...], preferred_element_type=jnp.float32).astype(
            jnp.bfloat16
        )
        swap_sums(slot).start()
        kept[slot] = jnp.dot(hid[mine, :], wd[...], preferred_element_type=jnp.float32).astype(
            jnp.bfloat16
        )

    def combine(i):
        slot = slot_of(i)
        swap_sums(slot).wait_recv()
        kept[slot] = (kept[slot].astype(jnp.float32) + pr[slot].astype(jnp.float32)).astype(
            jnp.bfloat16
        )

        @pl.when(i < layers)
        def _():
            across(order(i)).start()

    product(0)

    def step(i, carry):
        product(i)
        combine(i - 1)
        return carry

    lax.fori_loop(1, groups, step, 0)
    combine(groups - 1)

    def row_sum(zz):
        across(zz).wait_recv()
        return kept[zz * 2 + y].astype(jnp.float32) + rb[zz].astype(jnp.float32)

    def link(i, carry):
        zz = order(i)
        rising = zz > z
        fed = jnp.where(rising, z > 0, z + 1 < layers)
        total = row_sum(zz)

        @pl.when(fed)
        def _():
            chain(zz, zz, me).wait_recv()
            zb[zz] = (total + cbuf[zz].astype(jnp.float32)).astype(jnp.bfloat16)

        @pl.when(jnp.logical_not(fed))
        def _():
            zb[zz] = total.astype(jnp.bfloat16)

        nz = jnp.where(rising, z + 1, z - 1)
        landing = jnp.where(jnp.logical_and(nz == zz, jnp.logical_not(rising)), layers, zz)
        chain(zz, landing, here.chip(nz, y, x)).start()
        return carry

    lax.fori_loop(0, layers - 1, link, 0)
    total = row_sum(z)
    cbuf[layers + 1] = jnp.zeros(cbuf.shape[1:], jnp.bfloat16)

    @pl.when(z > 0)
    def _():
        chain(z, z, me).wait_recv()

    @pl.when(z + 1 < layers)
    def _():
        chain(z, layers, me).wait_recv()

    from_low = cbuf[jnp.where(z > 0, z, layers + 1)].astype(jnp.float32)
    from_high = cbuf[jnp.where(z + 1 < layers, layers, layers + 1)].astype(jnp.float32)
    acc = total + from_low + from_high
    ffn = acc.astype(jnp.bfloat16).astype(jnp.float32)
    out[...] = (mid[...].astype(jnp.float32) + ffn).astype(jnp.bfloat16)

    @pl.when(x == 0)
    def _():
        tail(groups - 1).wait_recv()

    def drain(a, carry):
        for b in range(2):
            for copy in across_x(a, b):
                copy.wait_send()
            forward(a * 2 + b).wait_send()
            swap_sums(a * 2 + b).wait_send()
            tail(a * 2 + b).wait_send()
        for copy in in_plane(a) + corner(a):
            copy.wait_send()
        spread(a).wait_send()
        across(a).wait_send()

        @pl.when(a != z)
        def _():
            answer(a).wait_send()
            chain(a, a, me).wait_send()

        @pl.when(jnp.logical_and(a <= z, z + 1 < layers))
        def _():
            line_up(a).wait_send()

        @pl.when(jnp.logical_and(a >= z, z > 0))
        def _():
            line_down(a).wait_send()

        @pl.when(a > 0)
        def _():
            for copy in along_z(a) + weights(a, 0):
                copy.wait_send()

        for copy in weights(a, 1):
            copy.wait_send()
        return carry

    lax.fori_loop(0, layers, drain, 0)


def vm(count):
    return [pl.BlockSpec(memory_space=pltpu.VMEM)] * count


def moving_rows(
    n,
    residual,
    queries,
    key_pairs,
    values,
    second_weight,
    head_gain,
    out_weight,
    norm_gain,
    up_weight,
    gate_weight,
    conv_weight,
    conv_bias,
    down_weight,
):
    rows, width = queries.shape
    half, model = residual.shape
    heads = second_weight.shape[0]
    depth, ff_local = up_weight.shape
    layers = n // 4
    groups = n // 2
    tiles = ff_local // VD
    wide = tile_count(tiles, groups) * VD
    rim = 16
    bf = jnp.bfloat16
    f32 = jnp.float32
    dma = pltpu.SemaphoreType.DMA

    def room(*dims):
        return pltpu.VMEM(dims, bf)

    return pl.pallas_call(
        functools.partial(layer_kernel, n),
        out_shape=jax.ShapeDtypeStruct((half, model), bf),
        in_specs=vm(3) + [pl.BlockSpec(memory_space=pltpu.SMEM)] + vm(9),
        out_specs=vm(1)[0],
        scratch_shapes=[
            room(n * depth, wide), room(n * depth, wide), room(wide, n * depth),
            room(half, model),
            room(layers, rows, VD), room(n * rows, VD), room(n * rows, VD),
            room(layers, rows, VD),
            pltpu.VMEM((layers, 2 * rows, 4 * rows), f32),
            room(rows, width), room(half, model), room(half, model),
            room(groups, rows, model), room(groups * rows, wide), room(groups * rows, wide),
            room(groups, rim, wide), room(groups + 1, rim, wide), room(rows, wide),
            room(groups, half, model), room(groups, half, model), room(groups, half, model),
            room(layers, half, model), room(layers, half, model), room(layers + 2, half, model),
            dma((3, layers)), dma((3, layers)), dma((6, layers)), dma((6, layers)),
            dma((layers,)), dma((layers,)), dma((2,)),
            dma((3, groups)), dma((3, groups)), dma((3, groups)), dma((3, groups)),
            dma((layers,)), dma((layers,)), dma((layers,)), dma((layers,)), dma((layers,)),
            dma((groups,)), dma((groups,)), dma((groups,)), dma((groups,)),
            dma((groups,)), dma((groups,)), dma((layers,)), dma((layers,)),
            dma((layers,)), dma((layers + 1,)),
        ],
        compiler_params=pltpu.CompilerParams(
            collective_id=0, has_side_effects=True, vmem_limit_bytes=VMEM_LIMIT
        ),
        name="layer_rows",
    )(
        queries, key_pairs, values, second_weight, head_gain.reshape(heads, VD),
        out_weight, residual, norm_gain[None, :], up_weight, gate_weight, down_weight,
        conv_weight, conv_bias.reshape(tiles, VD),
    )


def choose(n_sp, n_tp):
    def body(residual, queries, *rest):
        up_weight = rest[6]
        moves_rows = (
            n_tp == 2
            and n_sp % 4 == 0
            and rest[2].shape[0] == n_sp // 4
            and up_weight.shape[1] % VD == 0
            and up_weight.shape[1] // VD >= n_sp // 2
            and queries.shape[0] % 32 == 0
            and up_weight.shape[0] % VD == 0
            and rest[8].shape[0] <= 16
        )
        if moves_rows:
            return moving_rows(n_sp, residual, queries, *rest)
        return local(residual, queries, *rest)

    return body


def solution(mesh):
    return jax.shard_map(
        choose(mesh.shape["sp"], mesh.shape["tp"]),
        mesh=mesh,
        in_specs=(
            P(("sp", "tp"), None),
            P("sp", "tp"),
            P("sp", "tp"),
            P("sp", "tp"),
            P("tp"),
            P("tp"),
            P("tp", None),
            P(),
            P("sp", "tp"),
            P("sp", "tp"),
            P(None, "tp"),
            P("tp"),
            P("tp", "sp"),
        ),
        out_specs=P(("sp", "tp"), None),
        check_vma=False,
    )
```

```python
import functools

import jax
import jax.numpy as jnp
from jax import lax
from jax.experimental import pallas as pl
from jax.experimental.pallas import tpu as pltpu
from jax.sharding import PartitionSpec as P

MESH = pl.DeviceIdType.MESH
VMEM_LIMIT = 60 * 1024 * 1024

HD = 64
VD = 128


eps = 1e-05
neg_fill = -1e30
PIECES = 4


def from_behind(value, axis, steps):
    count = lax.axis_size(axis)
    leading, last = (max(0, -steps), min(count, count - steps))
    return lax.ppermute(value, axis, [(source, source + steps) for source in range(leading, last)])


def normalize(rows_in, gain):
    values_f = rows_in.astype(jnp.float32)
    scale_inv = lax.rsqrt(jnp.mean(values_f * values_f, axis=-1, keepdims=True) + eps)
    return (values_f * scale_inv * gain).astype(jnp.bfloat16)


def attend(queries, key_pairs, values, second_weight, head_gain):
    tok_rows = queries.shape[0]
    head_count = second_weight.shape[0]
    sp_index = lax.axis_index("sp")
    query = queries.reshape(tok_rows, head_count, 2, HD)
    query_pos = sp_index * tok_rows + jnp.arange(tok_rows)
    last_query = (sp_index + 1) * tok_rows
    initial = (
        jnp.full((head_count, 2, tok_rows), neg_fill, jnp.float32),
        jnp.zeros((head_count, 2, tok_rows), jnp.float32),
        jnp.zeros((head_count, 2, tok_rows, VD), jnp.float32),
    )
    key_piece = lax.all_gather(key_pairs, "sp", axis=0, tiled=True)
    value_piece = lax.all_gather(values, "sp", axis=0, tiled=True)
    piece_len = key_piece.shape[0]

    def compute(state_in):
        maxima, totals, weighted = state_in
        key_rows = key_piece.reshape(piece_len, head_count, 2, HD)
        value_rows = value_piece.reshape(piece_len, head_count, VD)
        scores = jnp.einsum(
            "qhmd,khmd->hmqk", query, key_rows, preferred_element_type=jnp.float32
        ) * HD ** (-0.5)
        visible = jnp.arange(piece_len)[None, :] <= query_pos[:, None]
        scores = jnp.where(visible, scores, neg_fill)
        new_max = jnp.maximum(maxima, jnp.max(scores, axis=-1))
        exp_scores = jnp.where(visible, jnp.exp(scores - new_max[..., None]), jnp.float32(0.0))
        totals = jnp.sum(exp_scores, axis=-1)
        weighted = jnp.einsum(
            "hmqk,khe->hmqe",
            exp_scores.astype(jnp.bfloat16),
            value_rows,
            preferred_element_type=jnp.float32,
        )
        return (new_max, totals, weighted)

    def keep_state(state_in):
        return state_in

    maxima, totals, weighted = lax.cond(jnp.int32(0) < last_query, compute, keep_state, initial)
    diff = (
        weighted[:, 0] / totals[:, 0, :, None]
        - second_weight[:, None, None] * weighted[:, 1] / totals[:, 1, :, None]
    )
    diff = jnp.transpose(diff, (1, 0, 2))
    scale_inv = lax.rsqrt(jnp.mean(diff * diff, axis=-1, keepdims=True) + eps)
    attended = (
        (diff * scale_inv * head_gain.reshape(head_count, VD) * 0.8)
        .reshape(tok_rows, head_count * VD)
        .astype(jnp.bfloat16)
    )
    return attended


def local(
    residual,
    queries,
    key_pairs,
    values,
    second_weight,
    head_gain,
    out_weight,
    norm_gain,
    up_weight,
    gate_weight,
    conv_weight,
    conv_bias,
    down_weight,
):
    tok_rows = queries.shape[0]
    ff_local = up_weight.shape[1]
    attended = attend(queries, key_pairs, values, second_weight, head_gain)
    proj = lax.psum_scatter(
        jnp.dot(attended, out_weight, preferred_element_type=jnp.float32).astype(jnp.bfloat16),
        "tp",
        scatter_dimension=0,
        tiled=True,
    )
    mid = (residual.astype(jnp.float32) + proj.astype(jnp.float32)).astype(jnp.bfloat16)
    normed_all = lax.all_gather(normalize(mid, norm_gain), "tp", axis=0, tiled=True)
    up_sum = jnp.dot(
        normed_all,
        lax.all_gather(up_weight, "sp", axis=0, tiled=True),
        preferred_element_type=jnp.float32,
    )
    gate_sum = jnp.dot(
        normed_all,
        lax.all_gather(gate_weight, "sp", axis=0, tiled=True),
        preferred_element_type=jnp.float32,
    )
    up_proj = up_sum.astype(jnp.bfloat16)
    gate_proj = gate_sum.astype(jnp.bfloat16)
    taps = conv_weight.shape[0]
    rim_rows = from_behind(up_proj[tok_rows - (taps - 1) :], "sp", 1)
    extended = jnp.concatenate((rim_rows, up_proj), axis=0)
    conv_out = jnp.zeros((tok_rows, ff_local), jnp.float32) + conv_bias[None, :]
    for tap in range(taps):
        conv_out = conv_out + conv_weight[tap][None, :] * extended[tap : tap + tok_rows].astype(
            jnp.float32
        )
    hidden = (jax.nn.silu(conv_out) * gate_proj.astype(jnp.float32)).astype(jnp.bfloat16)
    down_all = lax.all_gather(down_weight, "sp", axis=1, tiled=True)
    ffn_out = lax.psum_scatter(
        jnp.dot(hidden, down_all, preferred_element_type=jnp.float32).astype(jnp.bfloat16),
        "tp",
        scatter_dimension=0,
        tiled=True,
    )
    return (mid.astype(jnp.float32) + ffn_out.astype(jnp.float32)).astype(jnp.bfloat16)


def greet(n, me, t):
    barrier = pltpu.get_barrier_semaphore()

    def signal(k, carry):
        pl.semaphore_signal(
            barrier, inc=1, device_id={"sp": lax.rem(me + k, n)}, device_id_type=MESH
        )
        return carry

    lax.fori_loop(1, n, signal, 0)
    pl.semaphore_signal(barrier, inc=1, device_id={"tp": 1 - t}, device_id_type=MESH)
    pl.semaphore_wait(barrier, n)


def to_sp(src, dst, send, recv, dest):
    return pltpu.make_async_remote_copy(
        src_ref=src, dst_ref=dst, send_sem=send, recv_sem=recv,
        device_id={"sp": dest}, device_id_type=MESH,
    )


def to_tp(src, dst, send, recv, dest):
    return pltpu.make_async_remote_copy(
        src_ref=src, dst_ref=dst, send_sem=send, recv_sem=recv,
        device_id={"tp": dest}, device_id_type=MESH,
    )


def span(index, size):
    return pl.ds(pl.multiple_of(index * size, size), size)


def first_tile(group, tiles, groups):
    return group * tiles // groups


def tile_count(tiles, groups):
    return -(-tiles // groups)


class Place:
    def __init__(self, n):
        self.n = n
        self.layers = n // 4
        self.me = lax.axis_index("sp")
        self.t = lax.axis_index("tp")
        self.z = self.me // 4
        self.w = lax.rem(self.me, 4)
        self.y = self.w // 2
        self.x = lax.rem(self.w, 2)
        self.xn = self.z * 4 + self.y * 2 + (1 - self.x)
        self.yn = self.z * 4 + (1 - self.y) * 2 + self.x

    def ahead(self, a):
        return lax.rem(self.z + a, self.layers)

    def behind(self, a):
        return lax.rem(self.z - a + self.layers, self.layers)

    def chip(self, z, y, x):
        return z * 4 + y * 2 + x


def layer_kernel(
    n, q, k, v, sw, gain, ow, res, ngain, uw, gw, dw, cw, cb,
    out,
    wu, wg, wd, owb, resb, mid, qb, kb, vb, ob, sb, att, pbuf, prbuf,
    buf, up, gate, tails, halo, hid, pb, pr, kept, rb, zb, cbuf,
    lsem, zsend, zrecv, psend, precv, osend, orecv, tsem, wsend, wrecv, fsend, frecv,
    usend, dsend, lrecv, rsend, rrecv, csend, crecv, hsend, hrecv,
    xsend, xrecv, ysend, yrecv, ssend, srecv,
):
    here = Place(n)
    me, t, z, w, y, x = here.me, here.t, here.z, here.w, here.y, here.x
    layers = here.layers
    rows = q.shape[0]
    half = rows // 2
    depth = uw.shape[0]
    groups = n // 2
    tiles = uw.shape[1] // VD
    wide = wu.shape[1]
    chunk = 4 * rows

    def cols(h):
        return span(h, VD)

    def along_z(a):
        zz = here.ahead(a)
        dest = here.chip(zz, y, x)
        return (
            to_sp(k.at[:, cols(zz)], kb.at[span(me, rows)], zsend.at[0, a], zrecv.at[0, a], dest),
            to_sp(v.at[:, cols(zz)], vb.at[span(me, rows)], zsend.at[1, a], zrecv.at[1, a], dest),
            to_sp(q.at[:, cols(zz)], qb.at[z], zsend.at[2, a], zrecv.at[2, a], dest),
        )

    def in_plane(a):
        own = span(here.behind(a) * 4 + w, rows)
        return (
            to_sp(kb.at[own], kb.at[own], psend.at[0, a], precv.at[0, a], here.xn),
            to_sp(vb.at[own], vb.at[own], psend.at[1, a], precv.at[1, a], here.yn),
            to_sp(vb.at[own], vb.at[own], psend.at[2, a], precv.at[2, a], here.xn),
            to_sp(kb.at[own], kb.at[own], psend.at[3, a], precv.at[3, a], here.yn),
        )

    def corner(a):
        from_x = span(here.chip(here.behind(a), y, 1 - x), rows)
        from_y = span(here.chip(here.behind(a), 1 - y, x), rows)
        return (
            to_sp(kb.at[from_x], kb.at[from_x], psend.at[4, a], precv.at[4, a], here.yn),
            to_sp(vb.at[from_y], vb.at[from_y], psend.at[5, a], precv.at[5, a], here.xn),
        )

    most = wide - VD
    cuts = (slice(0, most), slice(most, wide))

    def begins(group):
        return first_tile(group, tiles, groups)

    def is_full(group):
        return begins(group + 1) - begins(group) == wide // VD

    own_group = z * 2 + y
    full = is_full(own_group)

    def target(a, b):
        return here.ahead(a), lax.rem(y + b, 2)

    def weights(a, b, cut):
        slot = a * 2 + b
        zz, yy = target(a, b)
        dest = here.chip(zz, yy, x)
        first = pl.multiple_of(begins(zz * 2 + yy) * VD + cuts[cut].start, VD)
        part = pl.ds(first, cuts[cut].stop - cuts[cut].start)
        place = span(me, depth)
        k = cut * 3
        return (
            to_sp(
                uw.at[:, part], wu.at[place, cuts[cut]],
                wsend.at[k, slot], wrecv.at[k, slot], dest,
            ),
            to_sp(
                gw.at[:, part], wg.at[place, cuts[cut]],
                wsend.at[k + 1, slot], wrecv.at[k + 1, slot], dest,
            ),
            to_sp(
                dw.at[part], wd.at[cuts[cut], place],
                wsend.at[k + 2, slot], wrecv.at[k + 2, slot], dest,
            ),
        )

    def across_x(a, b, cut):
        slot = a * 2 + b
        got = span(here.chip(here.behind(a), lax.rem(y + b, 2), x), depth)
        k = cut * 3
        return tuple(
            to_sp(ref, ref, fsend.at[k + i, slot], frecv.at[k + i, slot], here.xn)
            for i, ref in enumerate(
                (wu.at[got, cuts[cut]], wg.at[got, cuts[cut]], wd.at[cuts[cut], got])
            )
        )

    def both_cuts(make, whole, act):
        for copy in make(0):
            act(copy)

        @pl.when(whole)
        def _():
            for copy in make(1):
                act(copy)

    def whole_target(a, b):
        zz, yy = target(a, b)
        return is_full(zz * 2 + yy)

    def send_weights(a, b):
        both_cuts(lambda cut: weights(a, b, cut), whole_target(a, b), lambda c: c.start())

    def sent_weights(a, b):
        both_cuts(lambda cut: weights(a, b, cut), whole_target(a, b), lambda c: c.wait_send())

    def send_across(a, b):
        both_cuts(lambda cut: across_x(a, b, cut), full, lambda c: c.start())

    def sent_across(a, b):
        both_cuts(lambda cut: across_x(a, b, cut), full, lambda c: c.wait_send())

    def got_across(a, b):
        both_cuts(lambda cut: across_x(a, b, cut), full, lambda c: c.wait_recv())

    def pass_on(a, b):
        both_cuts(lambda cut: weights(a, b, cut), full, lambda c: c.wait_recv())
        send_across(a, b)

    def own_copies(cut):
        first = pl.multiple_of(begins(own_group) * VD + cuts[cut].start, VD)
        part = pl.ds(first, cuts[cut].stop - cuts[cut].start)
        place = span(me, depth)
        k = cut * 3
        return (
            pltpu.make_async_copy(uw.at[:, part], wu.at[place, cuts[cut]], lsem.at[k]),
            pltpu.make_async_copy(gw.at[:, part], wg.at[place, cuts[cut]], lsem.at[k + 1]),
            pltpu.make_async_copy(dw.at[part], wd.at[cuts[cut], place], lsem.at[k + 2]),
        )

    def side_copies():
        return (
            pltpu.make_async_copy(ow, owb, lsem.at[6]),
            pltpu.make_async_copy(res, resb, lsem.at[7]),
        )

    both_cuts(own_copies, full, lambda c: c.start())
    for copy in side_copies():
        copy.start()

    greet(n, me, t)

    for a in range(1, layers):
        for copy in along_z(a):
            copy.start()
    kb[span(me, rows), :] = k[:, cols(z)]
    vb[span(me, rows), :] = v[:, cols(z)]
    qb[z] = q[:, cols(z)]
    for copy in in_plane(0):
        copy.start()
    for a in range(1, layers):
        send_weights(a, 0)
    send_weights(0, 1)

    @pl.when(jnp.logical_not(full))
    def _():
        wu[:, cuts[1]] = jnp.zeros((wu.shape[0], VD), jnp.bfloat16)
        wg[:, cuts[1]] = jnp.zeros((wu.shape[0], VD), jnp.bfloat16)
        wd[cuts[1], :] = jnp.zeros((VD, wd.shape[1]), jnp.bfloat16)

    both_cuts(own_copies, full, lambda c: c.wait())

    def corner_stage(a):
        in_plane(a)[0].wait_recv()
        corner(a)[0].start()
        in_plane(a)[1].wait_recv()
        corner(a)[1].start()

    def stage(a, carry):
        copies = along_z(a)
        copies[0].wait_recv()
        copies[1].wait_recv()
        for copy in in_plane(a):
            copy.start()
        corner_stage(a - 1)
        return carry

    lax.fori_loop(1, layers, stage, 0)
    corner_stage(layers - 1)
    send_across(0, 0)

    def settle(a, carry):
        in_plane(a)[2].wait_recv()
        in_plane(a)[3].wait_recv()
        corner(a)[0].wait_recv()
        corner(a)[1].wait_recv()
        return carry

    lax.fori_loop(0, layers, settle, 0)
    for a in range(1, layers):
        along_z(a)[2].wait_recv()

    weight = sw[z]
    gain_row = gain[pl.ds(z, 1), :]
    lane = lax.broadcasted_iota(jnp.int32, (rows, VD), 1)

    def answer(i):
        return to_sp(
            ob.at[i], att.at[:, cols(z)], osend.at[i], orecv.at[z], here.chip(i, y, x)
        )

    def fold(op, value):
        total = value[:, :VD]
        for j in range(1, chunk // VD):
            total = op(total, value[:, j * VD : (j + 1) * VD])
        return total

    def block(i, carry):
        query = (qb[i].astype(jnp.float32) * HD ** (-0.5)).astype(jnp.bfloat16)
        zero = jnp.zeros_like(query)
        both = jnp.concatenate(
            (jnp.where(lane < HD, query, zero), jnp.where(lane < HD, zero, query)), axis=0
        )

        def scores_of(c):
            return lax.dot_general(
                both, kb[span(c, chunk), :], (((1,), (1,)), ((), ())),
                preferred_element_type=jnp.float32,
            )

        def score(c, peak):
            scores = scores_of(c)
            sb[c] = scores
            return jnp.maximum(peak, fold(jnp.maximum, scores))

        peak = lax.fori_loop(0, i, score, jnp.full((2 * rows, VD), neg_fill, jnp.float32))
        scores = scores_of(i)
        row = lax.broadcasted_iota(jnp.int32, scores.shape, 0)
        row = jnp.where(row < rows, row, row - rows)
        col = lax.broadcasted_iota(jnp.int32, scores.shape, 1)
        scores = jnp.where(col <= w * rows + row, scores, neg_fill)
        sb[i] = scores
        peak = jnp.maximum(peak, fold(jnp.maximum, scores))
        top = jnp.max(peak, axis=-1, keepdims=True)

        def weigh(c, state):
            total, acc = state
            exp_scores = jnp.exp(sb[c] - top)
            total = total + fold(jnp.add, exp_scores)
            acc = acc + jnp.dot(
                exp_scores.astype(jnp.bfloat16), vb[span(c, chunk), :],
                preferred_element_type=jnp.float32,
            )
            return total, acc

        blank = jnp.zeros((2 * rows, VD), jnp.float32)
        total, acc = lax.fori_loop(0, i + 1, weigh, (blank, blank))
        mean_v = acc / jnp.sum(total, axis=-1, keepdims=True)
        diff = mean_v[:rows] - weight * mean_v[rows:]
        inv = lax.rsqrt(jnp.mean(diff * diff, axis=-1, keepdims=True) + eps)
        result = (diff * inv * gain_row * 0.8).astype(jnp.bfloat16)

        @pl.when(i != z)
        def _():
            ob[i] = result
            answer(i).start()

        @pl.when(i == z)
        def _():
            att[:, cols(z)] = result

        @pl.when(i == 0)
        def _():
            pass_on(0, 1)

        @pl.when(i > 0)
        def _():
            pass_on(jnp.maximum(i, 1), 0)

        return carry

    lax.fori_loop(0, layers, block, 0)
    for a in range(1, layers):
        send_weights(a, 1)

    def answered(a, carry):
        h = here.behind(a)
        to_sp(ob.at[0], att.at[:, cols(h)], osend.at[0], orecv.at[h], me).wait_recv()
        return carry

    lax.fori_loop(1, layers, answered, 0)
    for copy in side_copies():
        copy.wait()
    mine = span(t, half)
    theirs = span(1 - t, half)
    pbuf[...] = jnp.dot(att[theirs, :], owb[...], preferred_element_type=jnp.float32).astype(
        jnp.bfloat16
    )
    swap = to_tp(pbuf, prbuf, tsem.at[0], tsem.at[1], 1 - t)
    swap.start()
    own = jnp.dot(att[mine, :], owb[...], preferred_element_type=jnp.float32).astype(jnp.bfloat16)
    swap.wait()
    proj = (own.astype(jnp.float32) + prbuf[...].astype(jnp.float32)).astype(jnp.bfloat16)
    mid_v = (resb[...].astype(jnp.float32) + proj.astype(jnp.float32)).astype(jnp.bfloat16)
    mid[...] = mid_v
    mid_f = mid_v.astype(jnp.float32)
    inv = lax.rsqrt(jnp.mean(mid_f * mid_f, axis=-1, keepdims=True) + eps)
    home = z * 2 + y
    buf[home, mine, :] = (mid_f * inv * ngain[...]).astype(jnp.bfloat16)
    halo[0] = jnp.zeros(halo.shape[1:], jnp.bfloat16)

    rim = tails.shape[1]
    taps = cw.shape[0]

    def line_up(zz):
        slot = zz * 2 + y
        dest = here.chip(jnp.minimum(z + 1, layers - 1), y, x)
        return to_sp(buf.at[slot, mine], buf.at[slot, mine], usend.at[zz], lrecv.at[zz], dest)

    def line_down(zz):
        slot = zz * 2 + y
        dest = here.chip(jnp.maximum(z - 1, 0), y, x)
        return to_sp(buf.at[slot, mine], buf.at[slot, mine], dsend.at[zz], lrecv.at[zz], dest)

    def spread(zz):
        slot = zz * 2 + y
        return to_sp(
            buf.at[slot, mine], buf.at[slot, mine], rsend.at[zz], rrecv.at[zz], here.yn
        )

    def spread_in(zz):
        slot = zz * 2 + 1 - y
        return to_sp(
            buf.at[slot, mine], buf.at[slot, mine], rsend.at[zz], rrecv.at[zz], here.yn
        )

    def forward(slot):
        return to_tp(
            buf.at[slot, mine], buf.at[slot, mine], csend.at[slot], crecv.at[slot], 1 - t
        )

    def arrived(slot):
        return to_tp(
            buf.at[slot, theirs], buf.at[slot, theirs], csend.at[slot], crecv.at[slot], 1 - t
        )

    def tail(j):
        return to_sp(tails.at[j], halo.at[j + 1], hsend.at[j], hrecv.at[j], here.xn)

    def compute(j):
        arrived(j).wait_recv()
        rows_in = buf[j]
        up_v = jnp.dot(rows_in, wu[...], preferred_element_type=jnp.float32).astype(jnp.bfloat16)
        up[span(j, rows), :] = up_v
        tails[j] = up_v[rows - rim :]
        tail(j).start()
        gate[span(j, rows), :] = jnp.dot(
            rows_in, wg[...], preferred_element_type=jnp.float32
        ).astype(jnp.bfloat16)

    @pl.when(z + 1 < layers)
    def _():
        line_up(z).start()

    @pl.when(z > 0)
    def _():
        line_down(z).start()

    spread(z).start()
    forward(home).start()

    def late(a, carry):
        pass_on(a, 1)
        return carry

    lax.fori_loop(1, layers, late, 0)

    def line_step(d):
        low, high = z - d, z + d

        @pl.when(low >= 0)
        def _():
            line_up(low).wait_recv()

            @pl.when(z + 1 < layers)
            def _():
                line_up(low).start()

            spread(low).start()
            forward(low * 2 + y).start()

        @pl.when(high < layers)
        def _():
            line_down(high).wait_recv()

            @pl.when(z > 0)
            def _():
                line_down(high).start()

            spread(high).start()
            forward(high * 2 + y).start()

    line_step(1)

    def crossed(a, carry):
        for b in range(2):
            got_across(a, b)
        return carry

    lax.fori_loop(0, layers, crossed, 0)

    def stage_rows(d, carry):
        @pl.when(jnp.logical_and(d > 0, d + 1 < layers))
        def _():
            line_step(d + 1)

        @pl.when(d == layers - 1)
        def _():
            product(layers - 2)
            product(groups - 2)
            combine(layers - 2)
            combine(groups - 2)

        low, high = z - d, z + d
        has_low = low >= 0
        has_high = jnp.logical_and(high < layers, d > 0)

        @pl.when(has_low)
        def _():
            compute(low * 2 + y)
            spread_in(low).wait_recv()
            forward(low * 2 + 1 - y).start()

        @pl.when(has_high)
        def _():
            compute(high * 2 + y)
            spread_in(high).wait_recv()
            forward(high * 2 + 1 - y).start()

        @pl.when(has_low)
        def _():
            compute(low * 2 + 1 - y)

        @pl.when(has_high)
        def _():
            compute(high * 2 + 1 - y)

        return carry

    start = first_tile(home, tiles, groups)
    real = (begins(home + 1) - start) * VD
    part = pl.ds(pl.multiple_of(start * VD, VD), wide)
    bias = jnp.concatenate([cb[pl.ds(start + j, 1), :] for j in range(wide // VD)], axis=1)

    below, above = z, layers - 1 - z

    def order(i):
        lead = jnp.abs(above - below)
        k = i - lead
        more_above = above >= below
        far = jnp.where(more_above, layers - 1 - i, i)
        near_even = jnp.where(more_above, k // 2, layers - 1 - k // 2)
        near_odd = jnp.where(more_above, layers - 1 - lead - k // 2, lead + k // 2)
        near = jnp.where(lax.rem(k + layers * 2, 2) == 0, near_even, near_odd)
        pick = jnp.where(i < lead, far, near)
        return jnp.where(i >= layers - 1, z, pick)

    def swap_sums(slot):
        return to_tp(pb.at[slot], pr.at[slot], xsend.at[slot], xrecv.at[slot], 1 - t)

    strip = out.shape[1] // PIECES
    strips = [slice(h * strip, (h + 1) * strip) for h in range(PIECES)]

    def across(zz, h):
        s = zz * PIECES + h
        return to_sp(
            kept.at[zz * 2 + 1 - y, :, strips[h]], rb.at[zz, :, strips[h]],
            ysend.at[s], yrecv.at[s], here.yn,
        )

    def chain(zz, landing, dest, h):
        return to_sp(
            zb.at[zz, :, strips[h]], cbuf.at[landing, :, strips[h]],
            ssend.at[zz * PIECES + h], srecv.at[landing * PIECES + h], dest,
        )

    def hidden(j):
        prior = jnp.where(x == 1, j, j - 1)

        @pl.when(prior >= 0)
        def _():
            tail(jnp.maximum(prior, 0)).wait_recv()

        edge = halo[prior + 1].astype(jnp.float32)
        now = up[span(j, rows), :].astype(jnp.float32)
        row = lax.broadcasted_iota(jnp.int32, now.shape, 0)
        conv = bias + cw[pl.ds(taps - 1, 1), part] * now
        for back in range(1, taps):
            moved = pltpu.roll(now, back, 0)
            for r in range(back):
                moved = jnp.where(row == r, edge[rim - back + r][None, :], moved)
            conv = conv + cw[pl.ds(taps - 1 - back, 1), part] * moved
        act = conv / (1.0 + jnp.exp(-conv)) * gate[span(j, rows), :].astype(jnp.float32)
        lane_of = lax.broadcasted_iota(jnp.int32, act.shape, 1)
        hid[...] = jnp.where(lane_of < real, act, 0.0).astype(jnp.bfloat16)

    def slot_of(i):
        side = jnp.where(i < layers, 1 - y, y)
        return order(lax.rem(i, layers)) * 2 + side

    def product(i):
        slot = slot_of(i)
        hidden(slot)
        pb[slot] = jnp.dot(hid[theirs, :], wd[...], preferred_element_type=jnp.float32).astype(
            jnp.bfloat16
        )
        swap_sums(slot).start()
        kept[slot] = jnp.dot(hid[mine, :], wd[...], preferred_element_type=jnp.float32).astype(
            jnp.bfloat16
        )

    def combine(i):
        slot = slot_of(i)
        swap_sums(slot).wait_recv()
        kept[slot] = (kept[slot].astype(jnp.float32) + pr[slot].astype(jnp.float32)).astype(
            jnp.bfloat16
        )

        @pl.when(i < layers)
        def _():
            for h in range(PIECES):
                across(order(i), h).start()

    def row_sum(zz, h):
        across(zz, h).wait_recv()
        return kept[zz * 2 + y, :, strips[h]].astype(jnp.float32) + rb[zz, :, strips[h]].astype(
            jnp.float32
        )

    def send_on(zz):
        rising = zz > z
        fed = jnp.where(rising, z > 0, z + 1 < layers)
        nz = jnp.where(rising, z + 1, z - 1)
        landing = jnp.where(jnp.logical_and(nz == zz, jnp.logical_not(rising)), layers, zz)
        for h in range(PIECES):
            total = row_sum(zz, h)

            @pl.when(fed)
            def _():
                chain(zz, zz, me, h).wait_recv()
                zb[zz, :, strips[h]] = (
                    total + cbuf[zz, :, strips[h]].astype(jnp.float32)
                ).astype(jnp.bfloat16)

            @pl.when(jnp.logical_not(fed))
            def _():
                zb[zz, :, strips[h]] = total.astype(jnp.bfloat16)

            chain(zz, landing, here.chip(nz, y, x), h).start()

    lax.fori_loop(0, layers, stage_rows, 0)
    at_end = jnp.logical_or(z == 0, z == layers - 1)

    @pl.when(at_end)
    def _():
        send_on(order(layers - 2))

    def later(i):
        skip = jnp.where(i < layers - 2, i, i + 1)
        return jnp.where(skip < groups - 2, skip, skip + 1)

    product(later(0))

    def step(i, carry):
        product(later(i))
        combine(later(i - 1))
        return carry

    lax.fori_loop(1, groups - 2, step, 0)
    combine(later(groups - 3))

    cbuf[layers + 1] = jnp.zeros(cbuf.shape[1:], jnp.bfloat16)

    def link(i, carry):
        @pl.when(jnp.logical_not(jnp.logical_and(at_end, i == layers - 2)))
        def _():
            send_on(order(i))

        return carry

    lax.fori_loop(0, layers - 1, link, 0)
    for h in range(PIECES):
        total = row_sum(z, h)

        @pl.when(z > 0)
        def _():
            chain(z, z, me, h).wait_recv()

        @pl.when(z + 1 < layers)
        def _():
            chain(z, layers, me, h).wait_recv()

        from_low = cbuf[jnp.where(z > 0, z, layers + 1), :, strips[h]]
        from_high = cbuf[jnp.where(z + 1 < layers, layers, layers + 1), :, strips[h]]
        total = total + from_low.astype(jnp.float32) + from_high.astype(jnp.float32)
        ffn = total.astype(jnp.bfloat16).astype(jnp.float32)
        out[:, strips[h]] = (mid[:, strips[h]].astype(jnp.float32) + ffn).astype(jnp.bfloat16)

    @pl.when(x == 0)
    def _():
        tail(groups - 1).wait_recv()

    def drain(a, carry):
        for b in range(2):
            sent_across(a, b)
            forward(a * 2 + b).wait_send()
            swap_sums(a * 2 + b).wait_send()
            tail(a * 2 + b).wait_send()
        for copy in in_plane(a) + corner(a):
            copy.wait_send()
        spread(a).wait_send()
        for h in range(PIECES):
            across(a, h).wait_send()

        @pl.when(a != z)
        def _():
            answer(a).wait_send()
            for h in range(PIECES):
                chain(a, a, me, h).wait_send()

        @pl.when(jnp.logical_and(a <= z, z + 1 < layers))
        def _():
            line_up(a).wait_send()

        @pl.when(jnp.logical_and(a >= z, z > 0))
        def _():
            line_down(a).wait_send()

        @pl.when(a > 0)
        def _():
            for copy in along_z(a):
                copy.wait_send()
            sent_weights(a, 0)

        sent_weights(a, 1)
        return carry

    lax.fori_loop(0, layers, drain, 0)


def vm(count):
    return [pl.BlockSpec(memory_space=pltpu.VMEM)] * count


def moving_rows(
    n,
    residual,
    queries,
    key_pairs,
    values,
    second_weight,
    head_gain,
    out_weight,
    norm_gain,
    up_weight,
    gate_weight,
    conv_weight,
    conv_bias,
    down_weight,
):
    rows, width = queries.shape
    half, model = residual.shape
    heads = second_weight.shape[0]
    depth, ff_local = up_weight.shape
    layers = n // 4
    groups = n // 2
    tiles = ff_local // VD
    wide = tile_count(tiles, groups) * VD
    rim = 16
    bf = jnp.bfloat16
    f32 = jnp.float32
    dma = pltpu.SemaphoreType.DMA

    away = [pl.BlockSpec(memory_space=pl.ANY)]

    def room(*dims):
        return pltpu.VMEM(dims, bf)

    return pl.pallas_call(
        functools.partial(layer_kernel, n),
        out_shape=jax.ShapeDtypeStruct((half, model), bf),
        in_specs=vm(3)
        + [pl.BlockSpec(memory_space=pltpu.SMEM)]
        + vm(1) + away * 2 + vm(1) + away * 3 + vm(2),
        out_specs=vm(1)[0],
        scratch_shapes=[
            room(n * depth, wide), room(n * depth, wide), room(wide, n * depth),
            room(width, model), room(half, model), room(half, model),
            room(layers, rows, VD), room(n * rows, VD), room(n * rows, VD),
            room(layers, rows, VD),
            pltpu.VMEM((layers, 2 * rows, 4 * rows), f32),
            room(rows, width), room(half, model), room(half, model),
            room(groups, rows, model), room(groups * rows, wide), room(groups * rows, wide),
            room(groups, rim, wide), room(groups + 1, rim, wide), room(rows, wide),
            room(groups, half, model), room(groups, half, model), room(groups, half, model),
            room(layers, half, model), room(layers, half, model), room(layers + 2, half, model),
            dma((8,)), dma((3, layers)), dma((3, layers)), dma((6, layers)), dma((6, layers)),
            dma((layers,)), dma((layers,)), dma((2,)),
            dma((6, groups)), dma((6, groups)), dma((6, groups)), dma((6, groups)),
            dma((layers,)), dma((layers,)), dma((layers,)), dma((layers,)), dma((layers,)),
            dma((groups,)), dma((groups,)), dma((groups,)), dma((groups,)),
            dma((groups,)), dma((groups,)),
            dma((layers * PIECES,)), dma((layers * PIECES,)),
            dma((layers * PIECES,)), dma(((layers + 1) * PIECES,)),
        ],
        compiler_params=pltpu.CompilerParams(
            collective_id=0, has_side_effects=True, vmem_limit_bytes=VMEM_LIMIT
        ),
        name="layer_rows",
    )(
        queries, key_pairs, values, second_weight, head_gain.reshape(heads, VD),
        out_weight, residual, norm_gain[None, :], up_weight, gate_weight, down_weight,
        conv_weight, conv_bias.reshape(tiles, VD),
    )


def choose(n_sp, n_tp):
    def body(residual, queries, *rest):
        up_weight = rest[6]
        moves_rows = (
            n_tp == 2
            and n_sp % 4 == 0
            and n_sp // 4 > 2
            and rest[2].shape[0] == n_sp // 4
            and up_weight.shape[1] % VD == 0
            and up_weight.shape[1] // VD > n_sp // 2
            and queries.shape[0] % 32 == 0
            and up_weight.shape[0] % VD == 0
            and rest[8].shape[0] <= 16
        )
        if moves_rows:
            return moving_rows(n_sp, residual, queries, *rest)
        return local(residual, queries, *rest)

    return body


def solution(mesh):
    return jax.shard_map(
        choose(mesh.shape["sp"], mesh.shape["tp"]),
        mesh=mesh,
        in_specs=(
            P(("sp", "tp"), None),
            P("sp", "tp"),
            P("sp", "tp"),
            P("sp", "tp"),
            P("tp"),
            P("tp"),
            P("tp", None),
            P(),
            P("sp", "tp"),
            P("sp", "tp"),
            P(None, "tp"),
            P("tp"),
            P("tp", "sp"),
        ),
        out_specs=P(("sp", "tp"), None),
        check_vma=False,
    )
```

```python
import functools

import jax
import jax.numpy as jnp
from jax import lax
from jax.experimental import pallas as pl
from jax.experimental.pallas import tpu as pltpu
from jax.sharding import PartitionSpec as P

MESH = pl.DeviceIdType.MESH
VMEM_LIMIT = 60 * 1024 * 1024

HD = 64
VD = 128


eps = 1e-05
neg_fill = -1e30
PIECES = 4


def from_behind(value, axis, steps):
    count = lax.axis_size(axis)
    leading, last = (max(0, -steps), min(count, count - steps))
    return lax.ppermute(value, axis, [(source, source + steps) for source in range(leading, last)])


def normalize(rows_in, gain):
    values_f = rows_in.astype(jnp.float32)
    scale_inv = lax.rsqrt(jnp.mean(values_f * values_f, axis=-1, keepdims=True) + eps)
    return (values_f * scale_inv * gain).astype(jnp.bfloat16)


def attend(queries, key_pairs, values, second_weight, head_gain):
    tok_rows = queries.shape[0]
    head_count = second_weight.shape[0]
    sp_index = lax.axis_index("sp")
    query = queries.reshape(tok_rows, head_count, 2, HD)
    query_pos = sp_index * tok_rows + jnp.arange(tok_rows)
    last_query = (sp_index + 1) * tok_rows
    initial = (
        jnp.full((head_count, 2, tok_rows), neg_fill, jnp.float32),
        jnp.zeros((head_count, 2, tok_rows), jnp.float32),
        jnp.zeros((head_count, 2, tok_rows, VD), jnp.float32),
    )
    key_piece = lax.all_gather(key_pairs, "sp", axis=0, tiled=True)
    value_piece = lax.all_gather(values, "sp", axis=0, tiled=True)
    piece_len = key_piece.shape[0]

    def compute(state_in):
        maxima, totals, weighted = state_in
        key_rows = key_piece.reshape(piece_len, head_count, 2, HD)
        value_rows = value_piece.reshape(piece_len, head_count, VD)
        scores = jnp.einsum(
            "qhmd,khmd->hmqk", query, key_rows, preferred_element_type=jnp.float32
        ) * HD ** (-0.5)
        visible = jnp.arange(piece_len)[None, :] <= query_pos[:, None]
        scores = jnp.where(visible, scores, neg_fill)
        new_max = jnp.maximum(maxima, jnp.max(scores, axis=-1))
        exp_scores = jnp.where(visible, jnp.exp(scores - new_max[..., None]), jnp.float32(0.0))
        totals = jnp.sum(exp_scores, axis=-1)
        weighted = jnp.einsum(
            "hmqk,khe->hmqe",
            exp_scores.astype(jnp.bfloat16),
            value_rows,
            preferred_element_type=jnp.float32,
        )
        return (new_max, totals, weighted)

    def keep_state(state_in):
        return state_in

    maxima, totals, weighted = lax.cond(jnp.int32(0) < last_query, compute, keep_state, initial)
    diff = (
        weighted[:, 0] / totals[:, 0, :, None]
        - second_weight[:, None, None] * weighted[:, 1] / totals[:, 1, :, None]
    )
    diff = jnp.transpose(diff, (1, 0, 2))
    scale_inv = lax.rsqrt(jnp.mean(diff * diff, axis=-1, keepdims=True) + eps)
    attended = (
        (diff * scale_inv * head_gain.reshape(head_count, VD) * 0.8)
        .reshape(tok_rows, head_count * VD)
        .astype(jnp.bfloat16)
    )
    return attended


def local(
    residual,
    queries,
    key_pairs,
    values,
    second_weight,
    head_gain,
    out_weight,
    norm_gain,
    up_weight,
    gate_weight,
    conv_weight,
    conv_bias,
    down_weight,
):
    tok_rows = queries.shape[0]
    ff_local = up_weight.shape[1]
    attended = attend(queries, key_pairs, values, second_weight, head_gain)
    proj = lax.psum_scatter(
        jnp.dot(attended, out_weight, preferred_element_type=jnp.float32).astype(jnp.bfloat16),
        "tp",
        scatter_dimension=0,
        tiled=True,
    )
    mid = (residual.astype(jnp.float32) + proj.astype(jnp.float32)).astype(jnp.bfloat16)
    normed_all = lax.all_gather(normalize(mid, norm_gain), "tp", axis=0, tiled=True)
    up_sum = jnp.dot(
        normed_all,
        lax.all_gather(up_weight, "sp", axis=0, tiled=True),
        preferred_element_type=jnp.float32,
    )
    gate_sum = jnp.dot(
        normed_all,
        lax.all_gather(gate_weight, "sp", axis=0, tiled=True),
        preferred_element_type=jnp.float32,
    )
    up_proj = up_sum.astype(jnp.bfloat16)
    gate_proj = gate_sum.astype(jnp.bfloat16)
    taps = conv_weight.shape[0]
    rim_rows = from_behind(up_proj[tok_rows - (taps - 1) :], "sp", 1)
    extended = jnp.concatenate((rim_rows, up_proj), axis=0)
    conv_out = jnp.zeros((tok_rows, ff_local), jnp.float32) + conv_bias[None, :]
    for tap in range(taps):
        conv_out = conv_out + conv_weight[tap][None, :] * extended[tap : tap + tok_rows].astype(
            jnp.float32
        )
    hidden = (jax.nn.silu(conv_out) * gate_proj.astype(jnp.float32)).astype(jnp.bfloat16)
    down_all = lax.all_gather(down_weight, "sp", axis=1, tiled=True)
    ffn_out = lax.psum_scatter(
        jnp.dot(hidden, down_all, preferred_element_type=jnp.float32).astype(jnp.bfloat16),
        "tp",
        scatter_dimension=0,
        tiled=True,
    )
    return (mid.astype(jnp.float32) + ffn_out.astype(jnp.float32)).astype(jnp.bfloat16)


def greet(n, me, t):
    barrier = pltpu.get_barrier_semaphore()

    def signal(k, carry):
        pl.semaphore_signal(
            barrier, inc=1, device_id={"sp": lax.rem(me + k, n)}, device_id_type=MESH
        )
        return carry

    lax.fori_loop(1, n, signal, 0)
    pl.semaphore_signal(barrier, inc=1, device_id={"tp": 1 - t}, device_id_type=MESH)
    pl.semaphore_wait(barrier, n)


def to_sp(src, dst, send, recv, dest):
    return pltpu.make_async_remote_copy(
        src_ref=src, dst_ref=dst, send_sem=send, recv_sem=recv,
        device_id={"sp": dest}, device_id_type=MESH,
    )


def to_tp(src, dst, send, recv, dest):
    return pltpu.make_async_remote_copy(
        src_ref=src, dst_ref=dst, send_sem=send, recv_sem=recv,
        device_id={"tp": dest}, device_id_type=MESH,
    )


def span(index, size):
    return pl.ds(pl.multiple_of(index * size, size), size)


def first_tile(group, tiles, groups):
    return group * tiles // groups


def tile_count(tiles, groups):
    return -(-tiles // groups)


class Place:
    def __init__(self, n):
        self.n = n
        self.layers = n // 4
        self.me = lax.axis_index("sp")
        self.t = lax.axis_index("tp")
        self.z = self.me // 4
        self.w = lax.rem(self.me, 4)
        self.y = self.w // 2
        self.x = lax.rem(self.w, 2)
        self.xn = self.z * 4 + self.y * 2 + (1 - self.x)
        self.yn = self.z * 4 + (1 - self.y) * 2 + self.x

    def ahead(self, a):
        return lax.rem(self.z + a, self.layers)

    def behind(self, a):
        return lax.rem(self.z - a + self.layers, self.layers)

    def chip(self, z, y, x):
        return z * 4 + y * 2 + x


def layer_kernel(
    n, q, k, v, sw, gain, ow, res, ngain, uw, gw, dw, cw, cb,
    out,
    wu, wg, wd, owb, resb, mid, qb, kb, vb, ob, sb, att, pbuf, prbuf,
    buf, up, gate, tails, halo, hid, part_sum, pr, rb, zb, cbuf,
    lsem, zsend, zrecv, psend, precv, osend, orecv, tsem, wsend, wrecv, fsend, frecv,
    usend, dsend, lrecv, rsend, rrecv, csend, crecv, hsend, hrecv,
    xsend, xrecv, ysend, yrecv, ssend, srecv,
):
    here = Place(n)
    me, t, z, w, y, x = here.me, here.t, here.z, here.w, here.y, here.x
    layers = here.layers
    rows = q.shape[0]
    half = rows // 2
    depth = uw.shape[0]
    groups = n // 2
    tiles = uw.shape[1] // VD
    wide = wu.shape[1]
    chunk = 4 * rows

    def cols(h):
        return span(h, VD)

    def along_z(a):
        zz = here.ahead(a)
        dest = here.chip(zz, y, x)
        return (
            to_sp(k.at[:, cols(zz)], kb.at[span(me, rows)], zsend.at[0, a], zrecv.at[0, a], dest),
            to_sp(v.at[:, cols(zz)], vb.at[span(me, rows)], zsend.at[1, a], zrecv.at[1, a], dest),
            to_sp(q.at[:, cols(zz)], qb.at[z], zsend.at[2, a], zrecv.at[2, a], dest),
        )

    def in_plane(a):
        own = span(here.behind(a) * 4 + w, rows)
        return (
            to_sp(kb.at[own], kb.at[own], psend.at[0, a], precv.at[0, a], here.xn),
            to_sp(vb.at[own], vb.at[own], psend.at[1, a], precv.at[1, a], here.yn),
            to_sp(vb.at[own], vb.at[own], psend.at[2, a], precv.at[2, a], here.xn),
            to_sp(kb.at[own], kb.at[own], psend.at[3, a], precv.at[3, a], here.yn),
        )

    def corner(a):
        from_x = span(here.chip(here.behind(a), y, 1 - x), rows)
        from_y = span(here.chip(here.behind(a), 1 - y, x), rows)
        return (
            to_sp(kb.at[from_x], kb.at[from_x], psend.at[4, a], precv.at[4, a], here.yn),
            to_sp(vb.at[from_y], vb.at[from_y], psend.at[5, a], precv.at[5, a], here.xn),
        )

    most = wide - VD
    cuts = (slice(0, most), slice(most, wide))

    def begins(group):
        return first_tile(group, tiles, groups)

    def is_full(group):
        return begins(group + 1) - begins(group) == wide // VD

    own_group = z * 2 + y
    full = is_full(own_group)

    def target(a, b):
        return here.ahead(a), lax.rem(y + b, 2)

    def weights(a, b, cut):
        slot = a * 2 + b
        zz, yy = target(a, b)
        dest = here.chip(zz, yy, x)
        first = pl.multiple_of(begins(zz * 2 + yy) * VD + cuts[cut].start, VD)
        part = pl.ds(first, cuts[cut].stop - cuts[cut].start)
        place = span(me, depth)
        k = cut * 3
        return (
            to_sp(
                uw.at[:, part], wu.at[place, cuts[cut]],
                wsend.at[k, slot], wrecv.at[k, slot], dest,
            ),
            to_sp(
                gw.at[:, part], wg.at[place, cuts[cut]],
                wsend.at[k + 1, slot], wrecv.at[k + 1, slot], dest,
            ),
            to_sp(
                dw.at[part], wd.at[cuts[cut], place],
                wsend.at[k + 2, slot], wrecv.at[k + 2, slot], dest,
            ),
        )

    def across_x(a, b, cut):
        slot = a * 2 + b
        got = span(here.chip(here.behind(a), lax.rem(y + b, 2), x), depth)
        k = cut * 3
        return tuple(
            to_sp(ref, ref, fsend.at[k + i, slot], frecv.at[k + i, slot], here.xn)
            for i, ref in enumerate(
                (wu.at[got, cuts[cut]], wg.at[got, cuts[cut]], wd.at[cuts[cut], got])
            )
        )

    def both_cuts(make, whole, act):
        for copy in make(0):
            act(copy)

        @pl.when(whole)
        def _():
            for copy in make(1):
                act(copy)

    def whole_target(a, b):
        zz, yy = target(a, b)
        return is_full(zz * 2 + yy)

    def send_weights(a, b):
        both_cuts(lambda cut: weights(a, b, cut), whole_target(a, b), lambda c: c.start())

    def sent_weights(a, b):
        both_cuts(lambda cut: weights(a, b, cut), whole_target(a, b), lambda c: c.wait_send())

    def send_across(a, b):
        both_cuts(lambda cut: across_x(a, b, cut), full, lambda c: c.start())

    def sent_across(a, b):
        both_cuts(lambda cut: across_x(a, b, cut), full, lambda c: c.wait_send())

    def got_across(a, b):
        both_cuts(lambda cut: across_x(a, b, cut), full, lambda c: c.wait_recv())

    def pass_on(a, b):
        both_cuts(lambda cut: weights(a, b, cut), full, lambda c: c.wait_recv())
        send_across(a, b)

    def own_copies(cut):
        first = pl.multiple_of(begins(own_group) * VD + cuts[cut].start, VD)
        part = pl.ds(first, cuts[cut].stop - cuts[cut].start)
        place = span(me, depth)
        k = cut * 3
        return (
            pltpu.make_async_copy(uw.at[:, part], wu.at[place, cuts[cut]], lsem.at[k]),
            pltpu.make_async_copy(gw.at[:, part], wg.at[place, cuts[cut]], lsem.at[k + 1]),
            pltpu.make_async_copy(dw.at[part], wd.at[cuts[cut], place], lsem.at[k + 2]),
        )

    def side_copies():
        return (
            pltpu.make_async_copy(ow, owb, lsem.at[6]),
            pltpu.make_async_copy(res, resb, lsem.at[7]),
        )

    both_cuts(own_copies, full, lambda c: c.start())
    for copy in side_copies():
        copy.start()

    greet(n, me, t)

    for a in range(1, layers):
        for copy in along_z(a):
            copy.start()
    kb[span(me, rows), :] = k[:, cols(z)]
    vb[span(me, rows), :] = v[:, cols(z)]
    qb[z] = q[:, cols(z)]
    for copy in in_plane(0):
        copy.start()
    send_weights(0, 1)
    send_weights(2, 0)

    @pl.when(jnp.logical_not(full))
    def _():
        wu[:, cuts[1]] = jnp.zeros((wu.shape[0], VD), jnp.bfloat16)
        wg[:, cuts[1]] = jnp.zeros((wu.shape[0], VD), jnp.bfloat16)
        wd[cuts[1], :] = jnp.zeros((VD, wd.shape[1]), jnp.bfloat16)

    both_cuts(own_copies, full, lambda c: c.wait())

    def corner_stage(a):
        in_plane(a)[0].wait_recv()
        corner(a)[0].start()
        in_plane(a)[1].wait_recv()
        corner(a)[1].start()

    def stage(a, carry):
        copies = along_z(a)
        copies[0].wait_recv()
        copies[1].wait_recv()
        for copy in in_plane(a):
            copy.start()
        corner_stage(a - 1)
        return carry

    lax.fori_loop(1, layers, stage, 0)
    corner_stage(layers - 1)
    send_weights(1, 0)
    send_weights(3, 0)
    send_across(0, 0)

    def settle(a, carry):
        in_plane(a)[2].wait_recv()
        in_plane(a)[3].wait_recv()
        corner(a)[0].wait_recv()
        corner(a)[1].wait_recv()
        return carry

    lax.fori_loop(0, layers, settle, 0)
    for a in range(1, layers):
        along_z(a)[2].wait_recv()

    weight = sw[z]
    gain_row = gain[pl.ds(z, 1), :]
    lane = lax.broadcasted_iota(jnp.int32, (rows, VD), 1)

    def answer(i):
        return to_sp(
            ob.at[i], att.at[:, cols(z)], osend.at[i], orecv.at[z], here.chip(i, y, x)
        )

    def fold(op, value):
        total = value[:, :VD]
        for j in range(1, chunk // VD):
            total = op(total, value[:, j * VD : (j + 1) * VD])
        return total

    def block(i, carry):
        query = (qb[i].astype(jnp.float32) * HD ** (-0.5)).astype(jnp.bfloat16)
        zero = jnp.zeros_like(query)
        both = jnp.concatenate(
            (jnp.where(lane < HD, query, zero), jnp.where(lane < HD, zero, query)), axis=0
        )

        def scores_of(c):
            return lax.dot_general(
                both, kb[span(c, chunk), :], (((1,), (1,)), ((), ())),
                preferred_element_type=jnp.float32,
            )

        def score(c, peak):
            scores = scores_of(c)
            sb[c] = scores
            return jnp.maximum(peak, fold(jnp.maximum, scores))

        peak = lax.fori_loop(0, i, score, jnp.full((2 * rows, VD), neg_fill, jnp.float32))
        scores = scores_of(i)
        row = lax.broadcasted_iota(jnp.int32, scores.shape, 0)
        row = jnp.where(row < rows, row, row - rows)
        col = lax.broadcasted_iota(jnp.int32, scores.shape, 1)
        scores = jnp.where(col <= w * rows + row, scores, neg_fill)
        sb[i] = scores
        peak = jnp.maximum(peak, fold(jnp.maximum, scores))
        top = jnp.max(peak, axis=-1, keepdims=True)

        def weigh(c, state):
            total, acc = state
            exp_scores = jnp.exp(sb[c] - top)
            total = total + fold(jnp.add, exp_scores)
            acc = acc + jnp.dot(
                exp_scores.astype(jnp.bfloat16), vb[span(c, chunk), :],
                preferred_element_type=jnp.float32,
            )
            return total, acc

        blank = jnp.zeros((2 * rows, VD), jnp.float32)
        total, acc = lax.fori_loop(0, i + 1, weigh, (blank, blank))
        mean_v = acc / jnp.sum(total, axis=-1, keepdims=True)
        diff = mean_v[:rows] - weight * mean_v[rows:]
        inv = lax.rsqrt(jnp.mean(diff * diff, axis=-1, keepdims=True) + eps)
        result = (diff * inv * gain_row * 0.8).astype(jnp.bfloat16)

        @pl.when(i != z)
        def _():
            ob[i] = result
            answer(i).start()

        @pl.when(i == z)
        def _():
            att[:, cols(z)] = result

        @pl.when(i == 0)
        def _():
            pass_on(0, 1)

        @pl.when(i > 0)
        def _():
            pass_on(jnp.maximum(i, 1), 0)

        return carry

    lax.fori_loop(0, layers, block, 0)
    for a in range(1, layers):
        send_weights(a, 1)

    def answered(a, carry):
        h = here.behind(a)
        to_sp(ob.at[0], att.at[:, cols(h)], osend.at[0], orecv.at[h], me).wait_recv()
        return carry

    lax.fori_loop(1, layers, answered, 0)
    for copy in side_copies():
        copy.wait()
    mine = span(t, half)
    theirs = span(1 - t, half)
    pbuf[...] = jnp.dot(att[theirs, :], owb[...], preferred_element_type=jnp.float32).astype(
        jnp.bfloat16
    )
    swap = to_tp(pbuf, prbuf, tsem.at[0], tsem.at[1], 1 - t)
    swap.start()
    own = jnp.dot(att[mine, :], owb[...], preferred_element_type=jnp.float32).astype(jnp.bfloat16)
    swap.wait()
    proj = (own.astype(jnp.float32) + prbuf[...].astype(jnp.float32)).astype(jnp.bfloat16)
    mid_v = (resb[...].astype(jnp.float32) + proj.astype(jnp.float32)).astype(jnp.bfloat16)
    mid[...] = mid_v
    mid_f = mid_v.astype(jnp.float32)
    inv = lax.rsqrt(jnp.mean(mid_f * mid_f, axis=-1, keepdims=True) + eps)
    home = z * 2 + y
    buf[home, mine, :] = (mid_f * inv * ngain[...]).astype(jnp.bfloat16)
    halo[0] = jnp.zeros(halo.shape[1:], jnp.bfloat16)

    rim = tails.shape[1]
    taps = cw.shape[0]

    strip = out.shape[1] // PIECES
    strips = [slice(h * strip, (h + 1) * strip) for h in range(PIECES)]

    def ahead_of(slot, h):
        return buf.at[slot, mine, strips[h]]

    def line_up(zz, h):
        ref = ahead_of(zz * 2 + y, h)
        s = zz * PIECES + h
        dest = here.chip(jnp.minimum(z + 1, layers - 1), y, x)
        return to_sp(ref, ref, usend.at[s], lrecv.at[s], dest)

    def line_down(zz, h):
        ref = ahead_of(zz * 2 + y, h)
        s = zz * PIECES + h
        dest = here.chip(jnp.maximum(z - 1, 0), y, x)
        return to_sp(ref, ref, dsend.at[s], lrecv.at[s], dest)

    def spread(zz, h):
        ref = ahead_of(zz * 2 + y, h)
        s = zz * PIECES + h
        return to_sp(ref, ref, rsend.at[s], rrecv.at[s], here.yn)

    def spread_in(zz, h):
        ref = ahead_of(zz * 2 + 1 - y, h)
        s = zz * PIECES + h
        return to_sp(ref, ref, rsend.at[s], rrecv.at[s], here.yn)

    def forward(slot, h):
        ref = ahead_of(slot, h)
        s = slot * PIECES + h
        return to_tp(ref, ref, csend.at[s], crecv.at[s], 1 - t)

    def arrived(slot, h):
        ref = buf.at[slot, theirs, strips[h]]
        s = slot * PIECES + h
        return to_tp(ref, ref, csend.at[s], crecv.at[s], 1 - t)

    def tail(j):
        return to_sp(tails.at[j], halo.at[j + 1], hsend.at[j], hrecv.at[j], here.xn)

    def compute(j):
        for h in range(PIECES):
            arrived(j, h).wait_recv()
        rows_in = buf[j]
        up_v = jnp.dot(rows_in, wu[...], preferred_element_type=jnp.float32).astype(jnp.bfloat16)
        up[span(j, rows), :] = up_v
        tails[j] = up_v[rows - rim :]
        tail(j).start()
        gate[span(j, rows), :] = jnp.dot(
            rows_in, wg[...], preferred_element_type=jnp.float32
        ).astype(jnp.bfloat16)

    @pl.when(z + 1 < layers)
    def _():
        for h in range(PIECES):
            line_up(z, h).start()

    @pl.when(z > 0)
    def _():
        for h in range(PIECES):
            line_down(z, h).start()

    for h in range(PIECES):
        spread(z, h).start()
        forward(home, h).start()

    def late(a, carry):
        pass_on(a, 1)
        return carry

    lax.fori_loop(1, layers, late, 0)

    def line_step(d):
        low, high = z - d, z + d
        for h in range(PIECES):

            @pl.when(low >= 0)
            def _():
                line_up(low, h).wait_recv()

                @pl.when(z + 1 < layers)
                def _():
                    line_up(low, h).start()

                spread(low, h).start()
                forward(low * 2 + y, h).start()

            @pl.when(high < layers)
            def _():
                line_down(high, h).wait_recv()

                @pl.when(z > 0)
                def _():
                    line_down(high, h).start()

                spread(high, h).start()
                forward(high * 2 + y, h).start()

    line_step(1)

    def crossed(a, carry):
        for b in range(2):
            got_across(a, b)
        return carry

    lax.fori_loop(0, layers, crossed, 0)

    def stage_rows(d, carry):
        @pl.when(jnp.logical_and(d > 0, d + 1 < layers))
        def _():
            line_step(d + 1)

        @pl.when(d == layers - 1)
        def _():
            product(layers - 2)
            product(groups - 2)
            combine(layers - 2)
            combine(groups - 2)

        low, high = z - d, z + d
        has_low = low >= 0
        has_high = jnp.logical_and(high < layers, d > 0)

        @pl.when(has_low)
        def _():
            compute(low * 2 + y)
            for h in range(PIECES):
                spread_in(low, h).wait_recv()
                forward(low * 2 + 1 - y, h).start()

        @pl.when(has_high)
        def _():
            compute(high * 2 + y)
            for h in range(PIECES):
                spread_in(high, h).wait_recv()
                forward(high * 2 + 1 - y, h).start()

        @pl.when(has_low)
        def _():
            compute(low * 2 + 1 - y)

        @pl.when(has_high)
        def _():
            compute(high * 2 + 1 - y)

        return carry

    start = first_tile(home, tiles, groups)
    real = (begins(home + 1) - start) * VD
    part = pl.ds(pl.multiple_of(start * VD, VD), wide)
    bias = jnp.concatenate([cb[pl.ds(start + j, 1), :] for j in range(wide // VD)], axis=1)

    below, above = z, layers - 1 - z

    def order(i):
        lead = jnp.abs(above - below)
        k = i - lead
        more_above = above >= below
        far = jnp.where(more_above, layers - 1 - i, i)
        near_even = jnp.where(more_above, k // 2, layers - 1 - k // 2)
        near_odd = jnp.where(more_above, layers - 1 - lead - k // 2, lead + k // 2)
        near = jnp.where(lax.rem(k + layers * 2, 2) == 0, near_even, near_odd)
        pick = jnp.where(i < lead, far, near)
        return jnp.where(i >= layers - 1, z, pick)

    def swap_sums(slot):
        return to_tp(
            part_sum.at[slot, theirs], pr.at[slot], xsend.at[slot], xrecv.at[slot], 1 - t
        )

    def across(zz, h):
        s = zz * PIECES + h
        return to_sp(
            part_sum.at[zz * 2 + 1 - y, mine, strips[h]], rb.at[zz, :, strips[h]],
            ysend.at[s], yrecv.at[s], here.yn,
        )

    def chain(zz, landing, dest, h):
        return to_sp(
            zb.at[zz, :, strips[h]], cbuf.at[landing, :, strips[h]],
            ssend.at[zz * PIECES + h], srecv.at[landing * PIECES + h], dest,
        )

    def hidden(j):
        prior = jnp.where(x == 1, j, j - 1)

        @pl.when(prior >= 0)
        def _():
            tail(jnp.maximum(prior, 0)).wait_recv()

        edge = halo[prior + 1].astype(jnp.float32)
        now = up[span(j, rows), :].astype(jnp.float32)
        row = lax.broadcasted_iota(jnp.int32, now.shape, 0)
        conv = bias + cw[pl.ds(taps - 1, 1), part] * now
        for back in range(1, taps):
            moved = pltpu.roll(now, back, 0)
            for r in range(back):
                moved = jnp.where(row == r, edge[rim - back + r][None, :], moved)
            conv = conv + cw[pl.ds(taps - 1 - back, 1), part] * moved
        act = conv / (1.0 + jnp.exp(-conv)) * gate[span(j, rows), :].astype(jnp.float32)
        lane_of = lax.broadcasted_iota(jnp.int32, act.shape, 1)
        hid[...] = jnp.where(lane_of < real, act, 0.0).astype(jnp.bfloat16)

    def slot_of(i):
        side = jnp.where(i < layers, 1 - y, y)
        return order(lax.rem(i, layers)) * 2 + side

    def product(i):
        slot = slot_of(i)
        hidden(slot)
        part_sum[slot] = jnp.dot(
            hid[...], wd[...], preferred_element_type=jnp.float32
        ).astype(jnp.bfloat16)
        swap_sums(slot).start()

    def combine(i):
        slot = slot_of(i)
        swap_sums(slot).wait_recv()
        kept = part_sum[slot, mine, :].astype(jnp.float32)
        part_sum[slot, mine, :] = (kept + pr[slot].astype(jnp.float32)).astype(jnp.bfloat16)

        @pl.when(i < layers)
        def _():
            for h in range(PIECES):
                across(order(i), h).start()

    def row_sum(zz, h):
        across(zz, h).wait_recv()
        kept = part_sum[zz * 2 + y, mine, strips[h]].astype(jnp.float32)
        return kept + rb[zz, :, strips[h]].astype(jnp.float32)

    def send_on(zz):
        rising = zz > z
        fed = jnp.where(rising, z > 0, z + 1 < layers)
        nz = jnp.where(rising, z + 1, z - 1)
        landing = jnp.where(jnp.logical_and(nz == zz, jnp.logical_not(rising)), layers, zz)
        for h in range(PIECES):
            total = row_sum(zz, h)

            @pl.when(fed)
            def _():
                chain(zz, zz, me, h).wait_recv()
                zb[zz, :, strips[h]] = (
                    total + cbuf[zz, :, strips[h]].astype(jnp.float32)
                ).astype(jnp.bfloat16)

            @pl.when(jnp.logical_not(fed))
            def _():
                zb[zz, :, strips[h]] = total.astype(jnp.bfloat16)

            chain(zz, landing, here.chip(nz, y, x), h).start()

    lax.fori_loop(0, layers, stage_rows, 0)
    at_end = jnp.logical_or(z == 0, z == layers - 1)

    @pl.when(at_end)
    def _():
        send_on(order(layers - 2))

    def later(i):
        skip = jnp.where(i < layers - 2, i, i + 1)
        return jnp.where(skip < groups - 2, skip, skip + 1)

    product(later(0))

    def step(i, carry):
        product(later(i))
        combine(later(i - 1))
        return carry

    lax.fori_loop(1, groups - 2, step, 0)
    combine(later(groups - 3))

    cbuf[layers + 1] = jnp.zeros(cbuf.shape[1:], jnp.bfloat16)

    def link(i, carry):
        @pl.when(jnp.logical_not(jnp.logical_and(at_end, i == layers - 2)))
        def _():
            send_on(order(i))

        return carry

    lax.fori_loop(0, layers - 1, link, 0)
    for h in range(PIECES):
        total = row_sum(z, h)

        @pl.when(z > 0)
        def _():
            chain(z, z, me, h).wait_recv()

        @pl.when(z + 1 < layers)
        def _():
            chain(z, layers, me, h).wait_recv()

        from_low = cbuf[jnp.where(z > 0, z, layers + 1), :, strips[h]]
        from_high = cbuf[jnp.where(z + 1 < layers, layers, layers + 1), :, strips[h]]
        total = total + from_low.astype(jnp.float32) + from_high.astype(jnp.float32)
        ffn = total.astype(jnp.bfloat16).astype(jnp.float32)
        out[:, strips[h]] = (mid[:, strips[h]].astype(jnp.float32) + ffn).astype(jnp.bfloat16)

    @pl.when(x == 0)
    def _():
        tail(groups - 1).wait_recv()

    def drain(a, carry):
        for b in range(2):
            sent_across(a, b)
            for h in range(PIECES):
                forward(a * 2 + b, h).wait_send()
            swap_sums(a * 2 + b).wait_send()
            tail(a * 2 + b).wait_send()
        for copy in in_plane(a) + corner(a):
            copy.wait_send()
        for h in range(PIECES):
            spread(a, h).wait_send()
        for h in range(PIECES):
            across(a, h).wait_send()

        @pl.when(a != z)
        def _():
            answer(a).wait_send()
            for h in range(PIECES):
                chain(a, a, me, h).wait_send()

        @pl.when(jnp.logical_and(a <= z, z + 1 < layers))
        def _():
            for h in range(PIECES):
                line_up(a, h).wait_send()

        @pl.when(jnp.logical_and(a >= z, z > 0))
        def _():
            for h in range(PIECES):
                line_down(a, h).wait_send()

        @pl.when(a > 0)
        def _():
            for copy in along_z(a):
                copy.wait_send()
            sent_weights(a, 0)

        sent_weights(a, 1)
        return carry

    lax.fori_loop(0, layers, drain, 0)


def vm(count):
    return [pl.BlockSpec(memory_space=pltpu.VMEM)] * count


def moving_rows(
    n,
    residual,
    queries,
    key_pairs,
    values,
    second_weight,
    head_gain,
    out_weight,
    norm_gain,
    up_weight,
    gate_weight,
    conv_weight,
    conv_bias,
    down_weight,
):
    rows, width = queries.shape
    half, model = residual.shape
    heads = second_weight.shape[0]
    depth, ff_local = up_weight.shape
    layers = n // 4
    groups = n // 2
    tiles = ff_local // VD
    wide = tile_count(tiles, groups) * VD
    rim = 16
    bf = jnp.bfloat16
    f32 = jnp.float32
    dma = pltpu.SemaphoreType.DMA

    away = [pl.BlockSpec(memory_space=pl.ANY)]

    def room(*dims):
        return pltpu.VMEM(dims, bf)

    return pl.pallas_call(
        functools.partial(layer_kernel, n),
        out_shape=jax.ShapeDtypeStruct((half, model), bf),
        in_specs=vm(3)
        + [pl.BlockSpec(memory_space=pltpu.SMEM)]
        + vm(1) + away * 2 + vm(1) + away * 3 + vm(2),
        out_specs=vm(1)[0],
        scratch_shapes=[
            room(n * depth, wide), room(n * depth, wide), room(wide, n * depth),
            room(width, model), room(half, model), room(half, model),
            room(layers, rows, VD), room(n * rows, VD), room(n * rows, VD),
            room(layers, rows, VD),
            pltpu.VMEM((layers, 2 * rows, 4 * rows), f32),
            room(rows, width), room(half, model), room(half, model),
            room(groups, rows, model), room(groups * rows, wide), room(groups * rows, wide),
            room(groups, rim, wide), room(groups + 1, rim, wide), room(rows, wide),
            room(groups, rows, model), room(groups, half, model),
            room(layers, half, model), room(layers, half, model), room(layers + 2, half, model),
            dma((8,)), dma((3, layers)), dma((3, layers)), dma((6, layers)), dma((6, layers)),
            dma((layers,)), dma((layers,)), dma((2,)),
            dma((6, groups)), dma((6, groups)), dma((6, groups)), dma((6, groups)),
            dma((layers * PIECES,)), dma((layers * PIECES,)), dma((layers * PIECES,)),
            dma((layers * PIECES,)), dma((layers * PIECES,)),
            dma((groups * PIECES,)), dma((groups * PIECES,)), dma((groups,)), dma((groups,)),
            dma((groups,)), dma((groups,)),
            dma((layers * PIECES,)), dma((layers * PIECES,)),
            dma((layers * PIECES,)), dma(((layers + 1) * PIECES,)),
        ],
        compiler_params=pltpu.CompilerParams(
            collective_id=0, has_side_effects=True, vmem_limit_bytes=VMEM_LIMIT
        ),
        name="layer_rows",
    )(
        queries, key_pairs, values, second_weight, head_gain.reshape(heads, VD),
        out_weight, residual, norm_gain[None, :], up_weight, gate_weight, down_weight,
        conv_weight, conv_bias.reshape(tiles, VD),
    )


def choose(n_sp, n_tp):
    def body(residual, queries, *rest):
        up_weight = rest[6]
        moves_rows = (
            n_tp == 2
            and n_sp % 4 == 0
            and n_sp // 4 > 2
            and rest[2].shape[0] == n_sp // 4
            and up_weight.shape[1] % VD == 0
            and up_weight.shape[1] // VD > n_sp // 2
            and queries.shape[0] % 32 == 0
            and up_weight.shape[0] % VD == 0
            and rest[8].shape[0] <= 16
        )
        if moves_rows:
            return moving_rows(n_sp, residual, queries, *rest)
        return local(residual, queries, *rest)

    return body


def solution(mesh):
    return jax.shard_map(
        choose(mesh.shape["sp"], mesh.shape["tp"]),
        mesh=mesh,
        in_specs=(
            P(("sp", "tp"), None),
            P("sp", "tp"),
            P("sp", "tp"),
            P("sp", "tp"),
            P("tp"),
            P("tp"),
            P("tp", None),
            P(),
            P("sp", "tp"),
            P("sp", "tp"),
            P(None, "tp"),
            P("tp"),
            P("tp", "sp"),
        ),
        out_specs=P(("sp", "tp"), None),
        check_vma=False,
    )
```

```python
import functools

import jax
import jax.numpy as jnp
from jax import lax
from jax.experimental import pallas as pl
from jax.experimental.pallas import tpu as pltpu
from jax.sharding import PartitionSpec as P

MESH = pl.DeviceIdType.MESH
VMEM_LIMIT = 60 * 1024 * 1024

HD = 64
VD = 128


eps = 1e-05
neg_fill = -1e30
PIECES = 4


def from_behind(value, axis, steps):
    count = lax.axis_size(axis)
    leading, last = (max(0, -steps), min(count, count - steps))
    return lax.ppermute(value, axis, [(source, source + steps) for source in range(leading, last)])


def normalize(rows_in, gain):
    values_f = rows_in.astype(jnp.float32)
    scale_inv = lax.rsqrt(jnp.mean(values_f * values_f, axis=-1, keepdims=True) + eps)
    return (values_f * scale_inv * gain).astype(jnp.bfloat16)


def attend(queries, key_pairs, values, second_weight, head_gain):
    tok_rows = queries.shape[0]
    head_count = second_weight.shape[0]
    sp_index = lax.axis_index("sp")
    query = queries.reshape(tok_rows, head_count, 2, HD)
    query_pos = sp_index * tok_rows + jnp.arange(tok_rows)
    last_query = (sp_index + 1) * tok_rows
    initial = (
        jnp.full((head_count, 2, tok_rows), neg_fill, jnp.float32),
        jnp.zeros((head_count, 2, tok_rows), jnp.float32),
        jnp.zeros((head_count, 2, tok_rows, VD), jnp.float32),
    )
    key_piece = lax.all_gather(key_pairs, "sp", axis=0, tiled=True)
    value_piece = lax.all_gather(values, "sp", axis=0, tiled=True)
    piece_len = key_piece.shape[0]

    def compute(state_in):
        maxima, totals, weighted = state_in
        key_rows = key_piece.reshape(piece_len, head_count, 2, HD)
        value_rows = value_piece.reshape(piece_len, head_count, VD)
        scores = jnp.einsum(
            "qhmd,khmd->hmqk", query, key_rows, preferred_element_type=jnp.float32
        ) * HD ** (-0.5)
        visible = jnp.arange(piece_len)[None, :] <= query_pos[:, None]
        scores = jnp.where(visible, scores, neg_fill)
        new_max = jnp.maximum(maxima, jnp.max(scores, axis=-1))
        exp_scores = jnp.where(visible, jnp.exp(scores - new_max[..., None]), jnp.float32(0.0))
        totals = jnp.sum(exp_scores, axis=-1)
        weighted = jnp.einsum(
            "hmqk,khe->hmqe",
            exp_scores.astype(jnp.bfloat16),
            value_rows,
            preferred_element_type=jnp.float32,
        )
        return (new_max, totals, weighted)

    def keep_state(state_in):
        return state_in

    maxima, totals, weighted = lax.cond(jnp.int32(0) < last_query, compute, keep_state, initial)
    diff = (
        weighted[:, 0] / totals[:, 0, :, None]
        - second_weight[:, None, None] * weighted[:, 1] / totals[:, 1, :, None]
    )
    diff = jnp.transpose(diff, (1, 0, 2))
    scale_inv = lax.rsqrt(jnp.mean(diff * diff, axis=-1, keepdims=True) + eps)
    attended = (
        (diff * scale_inv * head_gain.reshape(head_count, VD) * 0.8)
        .reshape(tok_rows, head_count * VD)
        .astype(jnp.bfloat16)
    )
    return attended


def local(
    residual,
    queries,
    key_pairs,
    values,
    second_weight,
    head_gain,
    out_weight,
    norm_gain,
    up_weight,
    gate_weight,
    conv_weight,
    conv_bias,
    down_weight,
):
    tok_rows = queries.shape[0]
    ff_local = up_weight.shape[1]
    attended = attend(queries, key_pairs, values, second_weight, head_gain)
    proj = lax.psum_scatter(
        jnp.dot(attended, out_weight, preferred_element_type=jnp.float32).astype(jnp.bfloat16),
        "tp",
        scatter_dimension=0,
        tiled=True,
    )
    mid = (residual.astype(jnp.float32) + proj.astype(jnp.float32)).astype(jnp.bfloat16)
    normed_all = lax.all_gather(normalize(mid, norm_gain), "tp", axis=0, tiled=True)
    up_sum = jnp.dot(
        normed_all,
        lax.all_gather(up_weight, "sp", axis=0, tiled=True),
        preferred_element_type=jnp.float32,
    )
    gate_sum = jnp.dot(
        normed_all,
        lax.all_gather(gate_weight, "sp", axis=0, tiled=True),
        preferred_element_type=jnp.float32,
    )
    up_proj = up_sum.astype(jnp.bfloat16)
    gate_proj = gate_sum.astype(jnp.bfloat16)
    taps = conv_weight.shape[0]
    rim_rows = from_behind(up_proj[tok_rows - (taps - 1) :], "sp", 1)
    extended = jnp.concatenate((rim_rows, up_proj), axis=0)
    conv_out = jnp.zeros((tok_rows, ff_local), jnp.float32) + conv_bias[None, :]
    for tap in range(taps):
        conv_out = conv_out + conv_weight[tap][None, :] * extended[tap : tap + tok_rows].astype(
            jnp.float32
        )
    hidden = (jax.nn.silu(conv_out) * gate_proj.astype(jnp.float32)).astype(jnp.bfloat16)
    down_all = lax.all_gather(down_weight, "sp", axis=1, tiled=True)
    ffn_out = lax.psum_scatter(
        jnp.dot(hidden, down_all, preferred_element_type=jnp.float32).astype(jnp.bfloat16),
        "tp",
        scatter_dimension=0,
        tiled=True,
    )
    return (mid.astype(jnp.float32) + ffn_out.astype(jnp.float32)).astype(jnp.bfloat16)


def greet(here):
    barrier = pltpu.get_barrier_semaphore()
    groups = here.n // 2

    def signal(k, carry):
        j = lax.rem(here.z * 2 + here.y + k, groups)
        dest = here.chip(j // 2, lax.rem(j, 2), here.x)
        pl.semaphore_signal(barrier, inc=1, device_id={"sp": dest}, device_id_type=MESH)
        return carry

    lax.fori_loop(1, groups, signal, 0)
    pl.semaphore_signal(barrier, inc=1, device_id={"sp": here.xn}, device_id_type=MESH)
    pl.semaphore_signal(barrier, inc=1, device_id={"tp": 1 - here.t}, device_id_type=MESH)
    pl.semaphore_wait(barrier, groups + 1)


def to_sp(src, dst, send, recv, dest):
    return pltpu.make_async_remote_copy(
        src_ref=src, dst_ref=dst, send_sem=send, recv_sem=recv,
        device_id={"sp": dest}, device_id_type=MESH,
    )


def to_tp(src, dst, send, recv, dest):
    return pltpu.make_async_remote_copy(
        src_ref=src, dst_ref=dst, send_sem=send, recv_sem=recv,
        device_id={"tp": dest}, device_id_type=MESH,
    )


def span(index, size):
    return pl.ds(pl.multiple_of(index * size, size), size)


def first_tile(group, tiles, groups):
    return group * tiles // groups


def tile_count(tiles, groups):
    return -(-tiles // groups)


class Place:
    def __init__(self, n):
        self.n = n
        self.layers = n // 4
        self.me = lax.axis_index("sp")
        self.t = lax.axis_index("tp")
        self.z = self.me // 4
        self.w = lax.rem(self.me, 4)
        self.y = self.w // 2
        self.x = lax.rem(self.w, 2)
        self.xn = self.z * 4 + self.y * 2 + (1 - self.x)
        self.yn = self.z * 4 + (1 - self.y) * 2 + self.x

    def ahead(self, a):
        return lax.rem(self.z + a, self.layers)

    def behind(self, a):
        return lax.rem(self.z - a + self.layers, self.layers)

    def chip(self, z, y, x):
        return z * 4 + y * 2 + x


def layer_kernel(
    n, q, k, v, sw, gain, ow, res, ngain, uw, gw, dw, cw, cb,
    out,
    wu, wg, wd, owb, resb, mid, qb, kb, vb, ob, sb, att, pbuf, prbuf,
    buf, up, gate, tails, halo, hid, part_sum, pr, rb, zb, cbuf,
    lsem, zsend, zrecv, psend, precv, osend, orecv, tsem, wsend, wrecv, fsend, frecv,
    usend, dsend, lrecv, rsend, rrecv, csend, crecv, hsend, hrecv,
    xsend, xrecv, ysend, yrecv, ssend, srecv,
):
    here = Place(n)
    me, t, z, w, y, x = here.me, here.t, here.z, here.w, here.y, here.x
    layers = here.layers
    rows = q.shape[0]
    half = rows // 2
    depth = uw.shape[0]
    groups = n // 2
    tiles = uw.shape[1] // VD
    wide = wu.shape[1]
    chunk = 4 * rows

    def cols(h):
        return span(h, VD)

    def along_z(a):
        zz = here.ahead(a)
        dest = here.chip(zz, y, x)
        return (
            to_sp(k.at[:, cols(zz)], kb.at[span(me, rows)], zsend.at[0, a], zrecv.at[0, a], dest),
            to_sp(v.at[:, cols(zz)], vb.at[span(me, rows)], zsend.at[1, a], zrecv.at[1, a], dest),
            to_sp(q.at[:, cols(zz)], qb.at[z], zsend.at[2, a], zrecv.at[2, a], dest),
        )

    def in_plane(a):
        own = span(here.behind(a) * 4 + w, rows)
        return (
            to_sp(kb.at[own], kb.at[own], psend.at[0, a], precv.at[0, a], here.xn),
            to_sp(vb.at[own], vb.at[own], psend.at[1, a], precv.at[1, a], here.yn),
            to_sp(vb.at[own], vb.at[own], psend.at[2, a], precv.at[2, a], here.xn),
            to_sp(kb.at[own], kb.at[own], psend.at[3, a], precv.at[3, a], here.yn),
        )

    def corner(a):
        from_x = span(here.chip(here.behind(a), y, 1 - x), rows)
        from_y = span(here.chip(here.behind(a), 1 - y, x), rows)
        return (
            to_sp(kb.at[from_x], kb.at[from_x], psend.at[4, a], precv.at[4, a], here.yn),
            to_sp(vb.at[from_y], vb.at[from_y], psend.at[5, a], precv.at[5, a], here.xn),
        )

    most = wide - VD
    cuts = (slice(0, most), slice(most, wide))

    def begins(group):
        return first_tile(group, tiles, groups)

    def is_full(group):
        return begins(group + 1) - begins(group) == wide // VD

    own_group = z * 2 + y
    full = is_full(own_group)

    def target(a, b):
        return here.ahead(a), lax.rem(y + b, 2)

    def weights(a, b, cut):
        slot = a * 2 + b
        zz, yy = target(a, b)
        dest = here.chip(zz, yy, x)
        first = pl.multiple_of(begins(zz * 2 + yy) * VD + cuts[cut].start, VD)
        part = pl.ds(first, cuts[cut].stop - cuts[cut].start)
        place = span(me, depth)
        k = cut * 3
        return (
            to_sp(
                uw.at[:, part], wu.at[place, cuts[cut]],
                wsend.at[k, slot], wrecv.at[k, slot], dest,
            ),
            to_sp(
                gw.at[:, part], wg.at[place, cuts[cut]],
                wsend.at[k + 1, slot], wrecv.at[k + 1, slot], dest,
            ),
            to_sp(
                dw.at[part], wd.at[cuts[cut], place],
                wsend.at[k + 2, slot], wrecv.at[k + 2, slot], dest,
            ),
        )

    def across_x(a, b, cut):
        slot = a * 2 + b
        got = span(here.chip(here.behind(a), lax.rem(y + b, 2), x), depth)
        k = cut * 3
        return tuple(
            to_sp(ref, ref, fsend.at[k + i, slot], frecv.at[k + i, slot], here.xn)
            for i, ref in enumerate(
                (wu.at[got, cuts[cut]], wg.at[got, cuts[cut]], wd.at[cuts[cut], got])
            )
        )

    def both_cuts(make, whole, act):
        for copy in make(0):
            act(copy)

        @pl.when(whole)
        def _():
            for copy in make(1):
                act(copy)

    def whole_target(a, b):
        zz, yy = target(a, b)
        return is_full(zz * 2 + yy)

    def send_weights(a, b):
        both_cuts(lambda cut: weights(a, b, cut), whole_target(a, b), lambda c: c.start())

    def sent_weights(a, b):
        both_cuts(lambda cut: weights(a, b, cut), whole_target(a, b), lambda c: c.wait_send())

    def send_across(a, b):
        both_cuts(lambda cut: across_x(a, b, cut), full, lambda c: c.start())

    def sent_across(a, b):
        both_cuts(lambda cut: across_x(a, b, cut), full, lambda c: c.wait_send())

    def got_across(a, b):
        both_cuts(lambda cut: across_x(a, b, cut), full, lambda c: c.wait_recv())

    def pass_on(a, b):
        both_cuts(lambda cut: weights(a, b, cut), full, lambda c: c.wait_recv())
        send_across(a, b)

    def own_copies(cut):
        first = pl.multiple_of(begins(own_group) * VD + cuts[cut].start, VD)
        part = pl.ds(first, cuts[cut].stop - cuts[cut].start)
        place = span(me, depth)
        k = cut * 3
        return (
            pltpu.make_async_copy(uw.at[:, part], wu.at[place, cuts[cut]], lsem.at[k]),
            pltpu.make_async_copy(gw.at[:, part], wg.at[place, cuts[cut]], lsem.at[k + 1]),
            pltpu.make_async_copy(dw.at[part], wd.at[cuts[cut], place], lsem.at[k + 2]),
        )

    def side_copies():
        return (
            pltpu.make_async_copy(ow, owb, lsem.at[6]),
            pltpu.make_async_copy(res, resb, lsem.at[7]),
        )

    both_cuts(own_copies, full, lambda c: c.start())
    for copy in side_copies():
        copy.start()

    greet(here)

    for a in range(1, layers):
        for copy in along_z(a):
            copy.start()
    kb[span(me, rows), :] = k[:, cols(z)]
    vb[span(me, rows), :] = v[:, cols(z)]
    qb[z] = q[:, cols(z)]
    for copy in in_plane(0):
        copy.start()
    send_weights(0, 1)
    send_weights(2, 0)

    @pl.when(jnp.logical_not(full))
    def _():
        wu[:, cuts[1]] = jnp.zeros((wu.shape[0], VD), jnp.bfloat16)
        wg[:, cuts[1]] = jnp.zeros((wu.shape[0], VD), jnp.bfloat16)
        wd[cuts[1], :] = jnp.zeros((VD, wd.shape[1]), jnp.bfloat16)

    both_cuts(own_copies, full, lambda c: c.wait())

    def corner_stage(a):
        in_plane(a)[0].wait_recv()
        corner(a)[0].start()
        in_plane(a)[1].wait_recv()
        corner(a)[1].start()

    def stage(a, carry):
        copies = along_z(a)
        copies[0].wait_recv()
        copies[1].wait_recv()
        for copy in in_plane(a):
            copy.start()
        corner_stage(a - 1)
        return carry

    lax.fori_loop(1, layers, stage, 0)
    corner_stage(layers - 1)
    send_weights(1, 0)
    send_weights(3, 0)
    send_across(0, 0)

    def settle(a, carry):
        in_plane(a)[2].wait_recv()
        in_plane(a)[3].wait_recv()
        corner(a)[0].wait_recv()
        corner(a)[1].wait_recv()
        return carry

    lax.fori_loop(0, layers, settle, 0)
    for a in range(1, layers):
        along_z(a)[2].wait_recv()

    weight = sw[z]
    gain_row = gain[pl.ds(z, 1), :]
    lane = lax.broadcasted_iota(jnp.int32, (rows, VD), 1)

    def answer(i):
        return to_sp(
            ob.at[i], att.at[:, cols(z)], osend.at[i], orecv.at[z], here.chip(i, y, x)
        )

    def fold(op, value):
        total = value[:, :VD]
        for j in range(1, chunk // VD):
            total = op(total, value[:, j * VD : (j + 1) * VD])
        return total

    def block(i, carry):
        query = (qb[i].astype(jnp.float32) * HD ** (-0.5)).astype(jnp.bfloat16)
        zero = jnp.zeros_like(query)
        both = jnp.concatenate(
            (jnp.where(lane < HD, query, zero), jnp.where(lane < HD, zero, query)), axis=0
        )

        def scores_of(c):
            return lax.dot_general(
                both, kb[span(c, chunk), :], (((1,), (1,)), ((), ())),
                preferred_element_type=jnp.float32,
            )

        def score(c, peak):
            scores = scores_of(c)
            sb[c] = scores
            return jnp.maximum(peak, fold(jnp.maximum, scores))

        peak = lax.fori_loop(0, i, score, jnp.full((2 * rows, VD), neg_fill, jnp.float32))
        scores = scores_of(i)
        row = lax.broadcasted_iota(jnp.int32, scores.shape, 0)
        row = jnp.where(row < rows, row, row - rows)
        col = lax.broadcasted_iota(jnp.int32, scores.shape, 1)
        scores = jnp.where(col <= w * rows + row, scores, neg_fill)
        sb[i] = scores
        peak = jnp.maximum(peak, fold(jnp.maximum, scores))
        top = jnp.max(peak, axis=-1, keepdims=True)

        def weigh(c, state):
            total, acc = state
            exp_scores = jnp.exp(sb[c] - top)
            total = total + fold(jnp.add, exp_scores)
            acc = acc + jnp.dot(
                exp_scores.astype(jnp.bfloat16), vb[span(c, chunk), :],
                preferred_element_type=jnp.float32,
            )
            return total, acc

        blank = jnp.zeros((2 * rows, VD), jnp.float32)
        total, acc = lax.fori_loop(0, i + 1, weigh, (blank, blank))
        mean_v = acc / jnp.sum(total, axis=-1, keepdims=True)
        diff = mean_v[:rows] - weight * mean_v[rows:]
        inv = lax.rsqrt(jnp.mean(diff * diff, axis=-1, keepdims=True) + eps)
        result = (diff * inv * gain_row * 0.8).astype(jnp.bfloat16)

        @pl.when(i != z)
        def _():
            ob[i] = result
            answer(i).start()

        @pl.when(i == z)
        def _():
            att[:, cols(z)] = result

        @pl.when(i == 0)
        def _():
            pass_on(0, 1)

        @pl.when(i > 0)
        def _():
            pass_on(jnp.maximum(i, 1), 0)

        return carry

    lax.fori_loop(0, layers, block, 0)
    for a in range(1, layers):
        send_weights(a, 1)

    def answered(a, carry):
        h = here.behind(a)
        to_sp(ob.at[0], att.at[:, cols(h)], osend.at[0], orecv.at[h], me).wait_recv()
        return carry

    lax.fori_loop(1, layers, answered, 0)
    for copy in side_copies():
        copy.wait()
    mine = span(t, half)
    theirs = span(1 - t, half)
    pbuf[...] = jnp.dot(att[theirs, :], owb[...], preferred_element_type=jnp.float32).astype(
        jnp.bfloat16
    )
    swap = to_tp(pbuf, prbuf, tsem.at[0], tsem.at[1], 1 - t)
    swap.start()
    own = jnp.dot(att[mine, :], owb[...], preferred_element_type=jnp.float32).astype(jnp.bfloat16)
    swap.wait()
    proj = (own.astype(jnp.float32) + prbuf[...].astype(jnp.float32)).astype(jnp.bfloat16)
    mid_v = (resb[...].astype(jnp.float32) + proj.astype(jnp.float32)).astype(jnp.bfloat16)
    mid[...] = mid_v
    mid_f = mid_v.astype(jnp.float32)
    inv = lax.rsqrt(jnp.mean(mid_f * mid_f, axis=-1, keepdims=True) + eps)
    home = z * 2 + y
    buf[home, mine, :] = (mid_f * inv * ngain[...]).astype(jnp.bfloat16)
    halo[0] = jnp.zeros(halo.shape[1:], jnp.bfloat16)

    rim = tails.shape[1]
    taps = cw.shape[0]

    strip = out.shape[1] // PIECES
    strips = [slice(h * strip, (h + 1) * strip) for h in range(PIECES)]

    def ahead_of(slot, h):
        return buf.at[slot, mine, strips[h]]

    def line_up(zz, h):
        ref = ahead_of(zz * 2 + y, h)
        s = zz * PIECES + h
        dest = here.chip(jnp.minimum(z + 1, layers - 1), y, x)
        return to_sp(ref, ref, usend.at[s], lrecv.at[s], dest)

    def line_down(zz, h):
        ref = ahead_of(zz * 2 + y, h)
        s = zz * PIECES + h
        dest = here.chip(jnp.maximum(z - 1, 0), y, x)
        return to_sp(ref, ref, dsend.at[s], lrecv.at[s], dest)

    def spread(zz, h):
        ref = ahead_of(zz * 2 + y, h)
        s = zz * PIECES + h
        return to_sp(ref, ref, rsend.at[s], rrecv.at[s], here.yn)

    def spread_in(zz, h):
        ref = ahead_of(zz * 2 + 1 - y, h)
        s = zz * PIECES + h
        return to_sp(ref, ref, rsend.at[s], rrecv.at[s], here.yn)

    def forward(slot, h):
        ref = ahead_of(slot, h)
        s = slot * PIECES + h
        return to_tp(ref, ref, csend.at[s], crecv.at[s], 1 - t)

    def arrived(slot, h):
        ref = buf.at[slot, theirs, strips[h]]
        s = slot * PIECES + h
        return to_tp(ref, ref, csend.at[s], crecv.at[s], 1 - t)

    def tail(j):
        return to_sp(tails.at[j], halo.at[j + 1], hsend.at[j], hrecv.at[j], here.xn)

    def compute(j):
        for h in range(PIECES):
            arrived(j, h).wait_recv()
        rows_in = buf[j]
        up_v = jnp.dot(rows_in, wu[...], preferred_element_type=jnp.float32).astype(jnp.bfloat16)
        up[span(j, rows), :] = up_v
        tails[j] = up_v[rows - rim :]
        tail(j).start()
        gate[span(j, rows), :] = jnp.dot(
            rows_in, wg[...], preferred_element_type=jnp.float32
        ).astype(jnp.bfloat16)

    @pl.when(z + 1 < layers)
    def _():
        for h in range(PIECES):
            line_up(z, h).start()

    @pl.when(z > 0)
    def _():
        for h in range(PIECES):
            line_down(z, h).start()

    for h in range(PIECES):
        spread(z, h).start()
        forward(home, h).start()

    def late(a, carry):
        pass_on(a, 1)
        return carry

    lax.fori_loop(1, layers, late, 0)

    def line_step(d):
        low, high = z - d, z + d
        for h in range(PIECES):

            @pl.when(low >= 0)
            def _():
                line_up(low, h).wait_recv()

                @pl.when(z + 1 < layers)
                def _():
                    line_up(low, h).start()

                spread(low, h).start()
                forward(low * 2 + y, h).start()

            @pl.when(high < layers)
            def _():
                line_down(high, h).wait_recv()

                @pl.when(z > 0)
                def _():
                    line_down(high, h).start()

                spread(high, h).start()
                forward(high * 2 + y, h).start()

    line_step(1)

    def crossed(a, carry):
        for b in range(2):
            got_across(a, b)
        return carry

    lax.fori_loop(0, layers, crossed, 0)

    def stage_rows(d, carry):
        @pl.when(jnp.logical_and(d > 0, d + 1 < layers))
        def _():
            line_step(d + 1)

        @pl.when(d == layers - 1)
        def _():
            product(layers - 2)
            product(groups - 2)
            combine(layers - 2)
            combine(groups - 2)

        low, high = z - d, z + d
        has_low = low >= 0
        has_high = jnp.logical_and(high < layers, d > 0)

        @pl.when(has_low)
        def _():
            compute(low * 2 + y)
            for h in range(PIECES):
                spread_in(low, h).wait_recv()
                forward(low * 2 + 1 - y, h).start()

        @pl.when(has_high)
        def _():
            compute(high * 2 + y)
            for h in range(PIECES):
                spread_in(high, h).wait_recv()
                forward(high * 2 + 1 - y, h).start()

        @pl.when(has_low)
        def _():
            compute(low * 2 + 1 - y)

        @pl.when(has_high)
        def _():
            compute(high * 2 + 1 - y)

        return carry

    start = first_tile(home, tiles, groups)
    real = (begins(home + 1) - start) * VD
    part = pl.ds(pl.multiple_of(start * VD, VD), wide)
    bias = jnp.concatenate([cb[pl.ds(start + j, 1), :] for j in range(wide // VD)], axis=1)

    below, above = z, layers - 1 - z

    def order(i):
        lead = jnp.abs(above - below)
        k = i - lead
        more_above = above >= below
        far = jnp.where(more_above, layers - 1 - i, i)
        near_even = jnp.where(more_above, k // 2, layers - 1 - k // 2)
        near_odd = jnp.where(more_above, layers - 1 - lead - k // 2, lead + k // 2)
        near = jnp.where(lax.rem(k + layers * 2, 2) == 0, near_even, near_odd)
        pick = jnp.where(i < lead, far, near)
        return jnp.where(i >= layers - 1, z, pick)

    def swap_sums(slot):
        return to_tp(
            part_sum.at[slot, theirs], pr.at[slot], xsend.at[slot], xrecv.at[slot], 1 - t
        )

    def across(zz, h):
        s = zz * PIECES + h
        return to_sp(
            part_sum.at[zz * 2 + 1 - y, mine, strips[h]], rb.at[zz, :, strips[h]],
            ysend.at[s], yrecv.at[s], here.yn,
        )

    def chain(zz, landing, dest, h):
        return to_sp(
            zb.at[zz, :, strips[h]], cbuf.at[landing, :, strips[h]],
            ssend.at[zz * PIECES + h], srecv.at[landing * PIECES + h], dest,
        )

    def hidden(j):
        prior = jnp.where(x == 1, j, j - 1)

        @pl.when(prior >= 0)
        def _():
            tail(jnp.maximum(prior, 0)).wait_recv()

        edge = halo[prior + 1].astype(jnp.float32)
        now = up[span(j, rows), :].astype(jnp.float32)
        row = lax.broadcasted_iota(jnp.int32, now.shape, 0)
        conv = bias + cw[pl.ds(taps - 1, 1), part] * now
        for back in range(1, taps):
            moved = pltpu.roll(now, back, 0)
            for r in range(back):
                moved = jnp.where(row == r, edge[rim - back + r][None, :], moved)
            conv = conv + cw[pl.ds(taps - 1 - back, 1), part] * moved
        act = conv / (1.0 + jnp.exp(-conv)) * gate[span(j, rows), :].astype(jnp.float32)
        lane_of = lax.broadcasted_iota(jnp.int32, act.shape, 1)
        hid[...] = jnp.where(lane_of < real, act, 0.0).astype(jnp.bfloat16)

    def slot_of(i):
        side = jnp.where(i < layers, 1 - y, y)
        return order(lax.rem(i, layers)) * 2 + side

    def product(i):
        slot = slot_of(i)
        hidden(slot)
        part_sum[slot] = jnp.dot(
            hid[...], wd[...], preferred_element_type=jnp.float32
        ).astype(jnp.bfloat16)
        swap_sums(slot).start()

    def combine(i):
        slot = slot_of(i)
        swap_sums(slot).wait_recv()
        kept = part_sum[slot, mine, :].astype(jnp.float32)
        part_sum[slot, mine, :] = (kept + pr[slot].astype(jnp.float32)).astype(jnp.bfloat16)

        @pl.when(i < layers)
        def _():
            for h in range(PIECES):
                across(order(i), h).start()

    def row_sum(zz, h):
        across(zz, h).wait_recv()
        kept = part_sum[zz * 2 + y, mine, strips[h]].astype(jnp.float32)
        return kept + rb[zz, :, strips[h]].astype(jnp.float32)

    def send_on(zz):
        rising = zz > z
        fed = jnp.where(rising, z > 0, z + 1 < layers)
        nz = jnp.where(rising, z + 1, z - 1)
        landing = jnp.where(jnp.logical_and(nz == zz, jnp.logical_not(rising)), layers, zz)
        for h in range(PIECES):
            total = row_sum(zz, h)

            @pl.when(fed)
            def _():
                chain(zz, zz, me, h).wait_recv()
                zb[zz, :, strips[h]] = (
                    total + cbuf[zz, :, strips[h]].astype(jnp.float32)
                ).astype(jnp.bfloat16)

            @pl.when(jnp.logical_not(fed))
            def _():
                zb[zz, :, strips[h]] = total.astype(jnp.bfloat16)

            chain(zz, landing, here.chip(nz, y, x), h).start()

    lax.fori_loop(0, layers, stage_rows, 0)
    at_end = jnp.logical_or(z == 0, z == layers - 1)

    @pl.when(at_end)
    def _():
        send_on(order(layers - 2))

    def later(i):
        skip = jnp.where(i < layers - 2, i, i + 1)
        return jnp.where(skip < groups - 2, skip, skip + 1)

    product(later(0))

    def step(i, carry):
        product(later(i))
        combine(later(i - 1))
        return carry

    lax.fori_loop(1, groups - 2, step, 0)
    combine(later(groups - 3))

    cbuf[layers + 1] = jnp.zeros(cbuf.shape[1:], jnp.bfloat16)

    def link(i, carry):
        @pl.when(jnp.logical_not(jnp.logical_and(at_end, i == layers - 2)))
        def _():
            send_on(order(i))

        return carry

    lax.fori_loop(0, layers - 1, link, 0)
    for h in range(PIECES):
        total = row_sum(z, h)

        @pl.when(z > 0)
        def _():
            chain(z, z, me, h).wait_recv()

        @pl.when(z + 1 < layers)
        def _():
            chain(z, layers, me, h).wait_recv()

        from_low = cbuf[jnp.where(z > 0, z, layers + 1), :, strips[h]]
        from_high = cbuf[jnp.where(z + 1 < layers, layers, layers + 1), :, strips[h]]
        total = total + from_low.astype(jnp.float32) + from_high.astype(jnp.float32)
        ffn = total.astype(jnp.bfloat16).astype(jnp.float32)
        out[:, strips[h]] = (mid[:, strips[h]].astype(jnp.float32) + ffn).astype(jnp.bfloat16)

    @pl.when(x == 0)
    def _():
        tail(groups - 1).wait_recv()

    def drain(a, carry):
        for b in range(2):
            sent_across(a, b)
            for h in range(PIECES):
                forward(a * 2 + b, h).wait_send()
            swap_sums(a * 2 + b).wait_send()
            tail(a * 2 + b).wait_send()
        for copy in in_plane(a) + corner(a):
            copy.wait_send()
        for h in range(PIECES):
            spread(a, h).wait_send()
        for h in range(PIECES):
            across(a, h).wait_send()

        @pl.when(a != z)
        def _():
            answer(a).wait_send()
            for h in range(PIECES):
                chain(a, a, me, h).wait_send()

        @pl.when(jnp.logical_and(a <= z, z + 1 < layers))
        def _():
            for h in range(PIECES):
                line_up(a, h).wait_send()

        @pl.when(jnp.logical_and(a >= z, z > 0))
        def _():
            for h in range(PIECES):
                line_down(a, h).wait_send()

        @pl.when(a > 0)
        def _():
            for copy in along_z(a):
                copy.wait_send()
            sent_weights(a, 0)

        sent_weights(a, 1)
        return carry

    lax.fori_loop(0, layers, drain, 0)


def vm(count):
    return [pl.BlockSpec(memory_space=pltpu.VMEM)] * count


def moving_rows(
    n,
    residual,
    queries,
    key_pairs,
    values,
    second_weight,
    head_gain,
    out_weight,
    norm_gain,
    up_weight,
    gate_weight,
    conv_weight,
    conv_bias,
    down_weight,
):
    rows, width = queries.shape
    half, model = residual.shape
    heads = second_weight.shape[0]
    depth, ff_local = up_weight.shape
    layers = n // 4
    groups = n // 2
    tiles = ff_local // VD
    wide = tile_count(tiles, groups) * VD
    rim = 16
    bf = jnp.bfloat16
    f32 = jnp.float32
    dma = pltpu.SemaphoreType.DMA

    away = [pl.BlockSpec(memory_space=pl.ANY)]

    def room(*dims):
        return pltpu.VMEM(dims, bf)

    return pl.pallas_call(
        functools.partial(layer_kernel, n),
        out_shape=jax.ShapeDtypeStruct((half, model), bf),
        in_specs=vm(3)
        + [pl.BlockSpec(memory_space=pltpu.SMEM)]
        + vm(1) + away * 2 + vm(1) + away * 3 + vm(2),
        out_specs=vm(1)[0],
        scratch_shapes=[
            room(n * depth, wide), room(n * depth, wide), room(wide, n * depth),
            room(width, model), room(half, model), room(half, model),
            room(layers, rows, VD), room(n * rows, VD), room(n * rows, VD),
            room(layers, rows, VD),
            pltpu.VMEM((layers, 2 * rows, 4 * rows), f32),
            room(rows, width), room(half, model), room(half, model),
            room(groups, rows, model), room(groups * rows, wide), room(groups * rows, wide),
            room(groups, rim, wide), room(groups + 1, rim, wide), room(rows, wide),
            room(groups, rows, model), room(groups, half, model),
            room(layers, half, model), room(layers, half, model), room(layers + 2, half, model),
            dma((8,)), dma((3, layers)), dma((3, layers)), dma((6, layers)), dma((6, layers)),
            dma((layers,)), dma((layers,)), dma((2,)),
            dma((6, groups)), dma((6, groups)), dma((6, groups)), dma((6, groups)),
            dma((layers * PIECES,)), dma((layers * PIECES,)), dma((layers * PIECES,)),
            dma((layers * PIECES,)), dma((layers * PIECES,)),
            dma((groups * PIECES,)), dma((groups * PIECES,)), dma((groups,)), dma((groups,)),
            dma((groups,)), dma((groups,)),
            dma((layers * PIECES,)), dma((layers * PIECES,)),
            dma((layers * PIECES,)), dma(((layers + 1) * PIECES,)),
        ],
        compiler_params=pltpu.CompilerParams(
            collective_id=0, has_side_effects=True, vmem_limit_bytes=VMEM_LIMIT
        ),
        name="layer_rows",
    )(
        queries, key_pairs, values, second_weight, head_gain.reshape(heads, VD),
        out_weight, residual, norm_gain[None, :], up_weight, gate_weight, down_weight,
        conv_weight, conv_bias.reshape(tiles, VD),
    )


def choose(n_sp, n_tp):
    def body(residual, queries, *rest):
        up_weight = rest[6]
        moves_rows = (
            n_tp == 2
            and n_sp % 4 == 0
            and n_sp // 4 > 2
            and rest[2].shape[0] == n_sp // 4
            and up_weight.shape[1] % VD == 0
            and up_weight.shape[1] // VD > n_sp // 2
            and queries.shape[0] % 32 == 0
            and up_weight.shape[0] % VD == 0
            and rest[8].shape[0] <= 16
        )
        if moves_rows:
            return moving_rows(n_sp, residual, queries, *rest)
        return local(residual, queries, *rest)

    return body


def solution(mesh):
    return jax.shard_map(
        choose(mesh.shape["sp"], mesh.shape["tp"]),
        mesh=mesh,
        in_specs=(
            P(("sp", "tp"), None),
            P("sp", "tp"),
            P("sp", "tp"),
            P("sp", "tp"),
            P("tp"),
            P("tp"),
            P("tp", None),
            P(),
            P("sp", "tp"),
            P("sp", "tp"),
            P(None, "tp"),
            P("tp"),
            P("tp", "sp"),
        ),
        out_specs=P(("sp", "tp"), None),
        check_vma=False,
    )
```
